32 devices in a mesh: sp: 16 (over z, y, x), tp: 2 (over core).
Axes of the slice: x: 2, y: 2, z: 4, core: 2. Of those that a mesh axis runs over, the one named last changes fastest.
Arguments:
- conv_value: bfloat16 [4096, 1024], P('sp', 'tp'), may hold values from -6 to 6
- conv_gate: bfloat16 [4096, 1024], P('sp', 'tp'), may hold values from -6 to 6
- taps: bfloat16 [31, 1024], P(None, 'tp'), may hold values from -1 to 1
- doc_ids: int32 [4096], P('sp'), may hold values from 0 to 3, never falling along the last dimension, each value on 1 to 2048 neighbouring positions
- gn_gain: float32 [1024], P('tp'), may hold values from 0.1 to 1.9
- gn_shift: float32 [1024], P('tp'), may hold values from -3 to 3
- conv_out: bfloat16 [1024, 2048], replicated, may hold values from -0.1875 to 0.1875
- residual: bfloat16 [4096, 2048], P(('sp', 'tp')), may hold values from -6 to 6
- norm_gain: float32 [2048], replicated, may hold values from 0.1 to 1.9
- routes: int32 [4096, 2], P(('sp', 'tp')), may hold values from 0 to 31, as said below
- route_weight: float32 [4096, 2], P(('sp', 'tp')), may hold values from 0.3 to 1.2
- expert_gate: bfloat16 [32, 2048, 512], P(('sp', 'tp')), may hold values from -0.125 to 0.125
- expert_up: bfloat16 [32, 2048, 512], P(('sp', 'tp')), may hold values from -0.125 to 0.125
- expert_down: bfloat16 [32, 512, 2048], P(('sp', 'tp')), may hold values from -0.25 to 0.25
- shared_gate: bfloat16 [2048, 512], replicated, may hold values from -0.125 to 0.125
- shared_up: bfloat16 [2048, 512], replicated, may hold values from -0.125 to 0.125
- shared_down: bfloat16 [512, 2048], replicated, may hold values from -0.25 to 0.25
Outputs:
- layer_out: bfloat16 [4096, 2048], P(('sp', 'tp'))
The draws below stay inside these ranges and needn't reach their ends.
Inputs may be any that keep to these rules, and one draw needn't show every extreme that they name: `routes`: each row names 2 different experts. The rows of one device name each expert at most 16 times, and one expert, the same for every device, exactly 16 times. `doc_ids`: numbers never fall from one position to the next.
All inputs are finite; a program needn't handle non-finite values.
Results may differ from the reference program's by a relative error of at most 0.014.
Values may be sent and summed in bfloat16 or wider, within the bound.
No kernel may reach another device: no remote copies, remote signals or barrier semaphores. Data moves between devices by JAX's collectives and lax.ppermute only.
A program may use at most 128 MiB of HBM per device.

```python
import math
import jax
import jax.numpy as jnp
import numpy as np
from jax import lax

D = 2048
CONV_DIM = 1024
GROUPS = 8
WIDTH = 31
EXPERT_DIM = 512
SHARED_DIM = 512
TOP_K = 2
TOK_SP = 256
TOK_DEV = 128
TOKENS = 4096
EXPERTS = 32
CAP = 16
DOCS = 4


def draw_routes(key, part):
    blocks = TOKENS // TOK_DEV
    pairs = EXPERTS // 2
    key_order = jax.random.fold_in(key, 11)
    key_tilt = jax.random.fold_in(key, 12)
    key_noise = jax.random.fold_in(key, 13)
    key_rows = jax.random.fold_in(key, 14)
    order = jax.random.permutation(key_order, EXPERTS).astype(jnp.int32)
    tilt = jax.random.randint(key_tilt, (pairs,), 0, CAP + 1)
    noise = jax.random.randint(key_noise, (blocks, pairs), -(CAP // 4), CAP // 4 + 1)
    first = jnp.clip(tilt[None, :] + noise, 0, CAP)
    first = first.at[:, 0].set(CAP)
    pair_counts = jnp.stack([first, CAP - first], axis=2).reshape(blocks, EXPERTS)
    counts = jnp.zeros((blocks, EXPERTS), jnp.int32).at[:, order].set(pair_counts.astype(jnp.int32))
    cumulative = jnp.cumsum(counts, axis=1).astype(jnp.int32)
    positions = jnp.arange(TOK_DEV * TOP_K, dtype=jnp.int32)
    expert_of = jax.vmap(lambda row: jnp.searchsorted(row, positions, side='right'))(cumulative).astype(jnp.int32)
    slots = expert_of.reshape(blocks, TOP_K, TOK_DEV).transpose(0, 2, 1)
    row_keys = jax.random.split(key_rows, blocks)
    shuffles = jax.vmap(lambda one_key: jax.random.permutation(one_key, TOK_DEV))(row_keys).astype(jnp.int32)
    shuffles = jnp.broadcast_to(shuffles[:, :, None], (blocks, TOK_DEV, TOP_K))
    shuffled = jnp.take_along_axis(slots, shuffles, axis=1)
    return shuffled.reshape(TOKENS, TOP_K).astype(jnp.int32)


def level_of(key, extent, shards, low, high):
    loudness = 1.0
    for dim, parts in shards:
        draws = jax.random.uniform(jax.random.fold_in(jax.random.fold_in(key, 6), dim), (parts,), jnp.float32, low / len(shards), high / len(shards))
        loudness = loudness * jnp.repeat(jnp.exp(draws), extent[dim] // parts).reshape((-1,) + (1,) * (len(extent) - 1 - dim))
    return loudness


def length_profile(count, total, reach, slope):
    weights = [(1 << 20) // math.isqrt(rank ** slope) + 1 for rank in range(2, count + 1)]
    rest, holding = total - reach - (count - 1), [1] * (count - 1)
    while rest > 0:
        candidates = [i for i in range(count - 1) if holding[i] < reach]
        pool, left = sum([weights[i] for i in candidates]), rest
        for i in candidates:
            more = min(reach - holding[i], max(1, left * weights[i] // pool), rest)
            holding[i] = holding[i] + more
            rest = rest - more
    return np.array([reach] + holding)


def uneven_parts(own_key, amount, total, bound, lean):
    if amount == 2:
        one = jax.random.randint(own_key, (), max(1, total - bound), min(bound, total - 1) + 1)
        return jnp.stack([one, total - one])
    sizes = jnp.asarray(length_profile(amount, total, bound, lean), jnp.int32)
    couples = (amount - 1) // 2
    giver, taker = sizes[1:1 + 2 * couples:2], sizes[2:2 + 2 * couples:2]
    room = jnp.minimum(giver - 1, bound - taker)
    moved = jax.random.randint(jax.random.fold_in(own_key, 1), (couples,), 0, 1 << 20) % (room + 1)
    sizes = sizes.at[1:1 + 2 * couples:2].set(giver - moved).at[2:2 + 2 * couples:2].set(taker + moved)
    return sizes[jax.random.permutation(jax.random.fold_in(own_key, 2), amount)]


def normal_values(own_key, dims, scale, most, cuts=(), kind=jnp.bfloat16):
    array = scale * jax.random.normal(own_key, dims, jnp.float32)
    if cuts:
        array = array * level_of(own_key, dims, cuts, -0.22, 0.18)
    return jnp.clip(array, -most, most).astype(kind)


def setup_inputs(seed: int = 0) -> dict:
    arg_keys = jax.random.split(jax.random.key(seed), 18)
    return {
        "conv_value": normal_values(arg_keys[0], (TOKENS, CONV_DIM), 1.0, 6.0, ((0, 16), (1, 2))),
        "conv_gate": normal_values(arg_keys[1], (TOKENS, CONV_DIM), 1.0, 6.0, ((0, 16), (1, 2))),
        "taps": normal_values(arg_keys[2], (WIDTH, CONV_DIM), WIDTH ** -0.5, 1.0, ((1, 2),)),
        "doc_ids": jnp.searchsorted(jnp.cumsum(uneven_parts(arg_keys[3], DOCS, TOKENS, 8 * TOK_SP, 1)), jnp.arange(TOKENS), side="right").astype(jnp.int32),
        "gn_gain": jnp.clip(1.0 + 0.18 * jax.random.normal(arg_keys[4], (CONV_DIM,), jnp.float32), 0.1, 1.9),
        "gn_shift": normal_values(arg_keys[5], (CONV_DIM,), 0.5, 3.0, ((0, 2),), jnp.float32),
        "conv_out": normal_values(arg_keys[6], (CONV_DIM, D), CONV_DIM ** -0.5, 0.1875),
        "residual": normal_values(arg_keys[7], (TOKENS, D), 1.0, 6.0, ((0, 32),)),
        "norm_gain": jnp.clip(1.0 + 0.18 * jax.random.normal(arg_keys[8], (D,), jnp.float32), 0.1, 1.9),
        "routes": draw_routes(jax.random.fold_in(arg_keys[17], 71), 0),
        "route_weight": jnp.clip(0.3 + 0.90000004 * jax.random.uniform(arg_keys[10], (TOKENS, TOP_K), jnp.float32) ** level_of(arg_keys[10], (TOKENS, TOP_K), ((0, 32),), -0.2, 0.2), 0.3, 1.2),
        "expert_gate": normal_values(arg_keys[11], (EXPERTS, D, EXPERT_DIM), D ** -0.5, 0.125, ((0, 32),)),
        "expert_up": normal_values(arg_keys[12], (EXPERTS, D, EXPERT_DIM), D ** -0.5, 0.125, ((0, 32),)),
        "expert_down": normal_values(arg_keys[13], (EXPERTS, EXPERT_DIM, D), EXPERT_DIM ** -0.5, 0.25, ((0, 32),)),
        "shared_gate": normal_values(arg_keys[14], (D, SHARED_DIM), D ** -0.5, 0.125),
        "shared_up": normal_values(arg_keys[15], (D, SHARED_DIM), D ** -0.5, 0.125),
        "shared_down": normal_values(arg_keys[16], (SHARED_DIM, D), SHARED_DIM ** -0.5, 0.25),
    }


epsilon = 1e-06

def route_rows(normed, routes, route_weight, expert_gate, expert_up, expert_down):
    blocks = TOKENS // TOK_DEV
    flat_routes = routes.reshape(blocks, TOK_DEV * TOP_K).astype(jnp.int32)
    onehot = (flat_routes[:, :, None] == jnp.arange(EXPERTS, dtype=jnp.int32)[None, None, :]).astype(jnp.int32)
    slot_index = (lax.optimization_barrier(jnp.sum(jnp.cumsum(onehot, axis=1) * onehot, axis=2)) - 1).astype(jnp.int32)
    block_index = jnp.broadcast_to(jnp.arange(blocks, dtype=jnp.int32)[:, None], flat_routes.shape)
    row_index = (block_index * TOK_DEV + jnp.arange(TOK_DEV * TOP_K, dtype=jnp.int32)[None, :] // TOP_K).astype(jnp.int32)
    slot_table = jnp.full((EXPERTS, blocks, CAP), TOKENS, jnp.int32).at[flat_routes, block_index, slot_index].set(row_index)
    weight_table = jnp.zeros((EXPERTS, blocks, CAP), jnp.float32).at[flat_routes, block_index, slot_index].set(route_weight.reshape(blocks, TOK_DEV * TOP_K).astype(jnp.float32))
    padded_rows = jnp.concatenate([normed, jnp.zeros((1, D), normed.dtype)], axis=0)

    def one_expert(routed_sum, pieces):
        table_rows, table_weights, gate_weight, up_weight, down_weight = pieces
        expert_rows = padded_rows[table_rows]
        gate_part = jnp.dot(expert_rows, gate_weight, preferred_element_type=jnp.float32)
        up_part = jnp.dot(expert_rows, up_weight, preferred_element_type=jnp.float32)
        hidden = (jax.nn.silu(gate_part) * up_part).astype(jnp.bfloat16)
        result = jnp.dot(hidden, down_weight, preferred_element_type=jnp.float32).astype(jnp.bfloat16)
        routed_sum = routed_sum.at[table_rows].add(table_weights[:, None] * result.astype(jnp.float32), mode='drop')
        return (routed_sum, None)
    routed, _ = lax.scan(one_expert, jnp.zeros((TOKENS, D), jnp.float32), (slot_table.reshape(EXPERTS, blocks * CAP), weight_table.reshape(EXPERTS, blocks * CAP), expert_gate, expert_up, expert_down))
    return routed

def reference(conv_value, conv_gate, taps, doc_ids, gn_gain, gn_shift, conv_out, residual, norm_gain, routes, route_weight, expert_gate, expert_up, expert_down, shared_gate, shared_up, shared_down):
    glu = (conv_value.astype(jnp.float32) * jax.nn.sigmoid(conv_gate.astype(jnp.float32))).astype(jnp.bfloat16)
    padded_glu = jnp.pad(glu, ((WIDTH - 1, 0), (0, 0)))
    padded_ids = jnp.pad(doc_ids, (WIDTH - 1, 0), constant_values=-1)
    conv_sum = jnp.zeros((TOKENS, CONV_DIM), jnp.float32)
    for offset in range(WIDTH):
        same_doc = (padded_ids[offset:offset + TOKENS] == doc_ids)[:, None]
        tap_term = taps[offset].astype(jnp.float32)[None, :] * padded_glu[offset:offset + TOKENS].astype(jnp.float32)
        conv_sum = conv_sum + jnp.where(same_doc, tap_term, 0.0)
    grouped = conv_sum.reshape(TOKENS, GROUPS, CONV_DIM // GROUPS)
    group_mean = lax.optimization_barrier(jnp.mean(grouped, axis=-1, keepdims=True))
    centered = grouped - group_mean
    group_var = lax.optimization_barrier(jnp.mean(centered * centered, axis=-1, keepdims=True))
    normalized = (centered * lax.rsqrt(group_var + epsilon)).reshape(TOKENS, CONV_DIM)
    conv_act = jax.nn.silu(normalized * gn_gain + gn_shift).astype(jnp.bfloat16)
    projected = jnp.dot(conv_act, conv_out, preferred_element_type=jnp.float32)
    stream = (residual.astype(jnp.float32) + projected).astype(jnp.bfloat16)
    stream_wide = stream.astype(jnp.float32)
    normed = (stream_wide * lax.rsqrt(lax.optimization_barrier(jnp.mean(stream_wide * stream_wide, axis=-1, keepdims=True)) + epsilon) * norm_gain).astype(jnp.bfloat16)
    shared_hidden = (jax.nn.silu(jnp.dot(normed, shared_gate, preferred_element_type=jnp.float32)) * jnp.dot(normed, shared_up, preferred_element_type=jnp.float32)).astype(jnp.bfloat16)
    shared_out = jnp.dot(shared_hidden, shared_down, preferred_element_type=jnp.float32)
    routed = route_rows(normed, routes, route_weight, expert_gate, expert_up, expert_down)
    return (stream_wide + shared_out + routed).astype(jnp.bfloat16)
```

```python
import functools

import jax
import jax.numpy as jnp
from jax import lax
from jax.experimental import pallas as pl
from jax.experimental.pallas import tpu as pltpu
from jax.sharding import Mesh
from jax.sharding import PartitionSpec as P

LANES = 128


epsilon = 1e-06

HALF = ("sp", "tp")
LINE = ("half", "sp")

F32, BF16, I32 = jnp.float32, jnp.bfloat16, jnp.int32


def from_behind(x, axis, by):
    peers = lax.axis_size(axis)
    pairs = [(i, i + by) for i in range(peers) if 0 <= i + by < peers]
    return lax.ppermute(x, axis, pairs)


def to_mirror(x):
    return lax.ppermute(x, "half", [(0, 1), (1, 0)])


def call(body, outs, scratch=(), flops=0, moved=0):
    return pl.pallas_call(
        body,
        out_shape=outs,
        scratch_shapes=list(scratch),
        cost_estimate=pl.CostEstimate(flops=flops, bytes_accessed=moved, transcendentals=0),
    )


def glu_of(value, gate):
    return (value.astype(F32) * jax.nn.sigmoid(gate.astype(F32))).astype(BF16)


def conv_body(
    value_ref, gate_ref, edge_ref, ids_ref, taps_ref, gain_ref, shift_ref, out_ref, glu, ids
):
    positions, channels = value_ref.shape
    width = taps_ref.shape[0]
    rim = edge_ref.shape[0]
    blocks = channels // LANES
    rows = 32
    ids[pl.ds(0, rim), :] = edge_ref[:, pl.ds(channels, LANES)].astype(F32)
    ids[pl.ds(rim, positions), :] = ids_ref[...]
    for c in range(blocks):
        lanes = pl.ds(c * LANES, LANES)
        glu[c, pl.ds(0, rim), :] = edge_ref[:, lanes].astype(F32)
        glu[c, pl.ds(rim, positions), :] = glu_of(value_ref[:, lanes], gate_ref[:, lanes]).astype(
            F32
        )

    def chunk(index, carry):
        row = pl.multiple_of(index * rows, rows)
        here = ids[pl.ds(row + rim, rows), :]
        total = [jnp.zeros((rows, LANES), F32) for _ in range(blocks)]
        for tap in range(width):
            past = row + (rim - width + 1 + tap)
            same = ids[pl.ds(past, rows), :] == here
            for c in range(blocks):
                weight = taps_ref[pl.ds(tap, 1), pl.ds(c * LANES, LANES)]
                term = weight * glu[c, pl.ds(past, rows), :]
                total[c] = total[c] + jnp.where(same, term, 0.0)
        for c in range(blocks):
            lanes = pl.ds(c * LANES, LANES)
            centered = total[c] - jnp.mean(total[c], axis=-1, keepdims=True)
            spread = jnp.mean(centered * centered, axis=-1, keepdims=True)
            scaled = centered * lax.rsqrt(spread + epsilon)
            out_ref[pl.ds(row, rows), lanes] = jax.nn.silu(
                scaled * gain_ref[:, lanes] + shift_ref[:, lanes]
            ).astype(BF16)
        return carry

    lax.fori_loop(0, positions // rows, chunk, 0)


def convolve(value, gate, edge, ids, taps, gain, shift):
    positions, channels = value.shape
    rim = edge.shape[0]
    return call(
        conv_body,
        jax.ShapeDtypeStruct(value.shape, BF16),
        scratch=[
            pltpu.VMEM((channels // LANES, rim + positions, LANES), F32),
            pltpu.VMEM((rim + positions, LANES), F32),
        ],
        flops=6_000_000_000,
        moved=3 * value.size * 2,
    )(value, gate, edge, ids, taps, gain, shift)


def selection(routes, first, experts, capacity, rows):
    top, tokens = routes.shape
    routes = routes.astype(I32)
    names = lax.broadcasted_iota(I32, (experts, tokens), 0)
    earlier = lax.broadcasted_iota(I32, (tokens, tokens), 0) < lax.broadcasted_iota(
        I32, (tokens, tokens), 1
    )
    earlier = earlier.astype(F32).astype(BF16)
    index = lax.broadcasted_iota(I32, (rows, tokens), 0)
    used = jnp.zeros((experts, 1), F32)
    picks = []
    for k in range(top):
        route = routes[k : k + 1, :]
        chosen = (names == route).astype(F32)
        before = jnp.dot(chosen.astype(BF16), earlier, preferred_element_type=F32) + used
        slot = jnp.sum(chosen * before, axis=0, keepdims=True).astype(I32)
        picks.append(index == (route - first) * capacity + slot)
        used = used + jnp.sum(chosen, axis=1, keepdims=True)
    return picks


def project_body(
    shape_of, keep, first_ref, act_ref, weight_ref, residual_ref, gain_ref, routes_ref, *outs
):
    experts, capacity = shape_of
    parcel_ref = outs[0]
    parts, _, depth = act_ref.shape
    projected = jnp.dot(act_ref[0], weight_ref[pl.ds(0, depth), :], preferred_element_type=F32)
    for part in range(1, parts):
        projected = projected + jnp.dot(
            act_ref[part], weight_ref[pl.ds(part * depth, depth), :], preferred_element_type=F32
        )
    stream = (residual_ref[...].astype(F32) + projected).astype(BF16)
    wide = stream.astype(F32)
    normed = (
        wide * lax.rsqrt(jnp.mean(wide * wide, axis=-1, keepdims=True) + epsilon) * gain_ref[...]
    ).astype(BF16)
    if keep:
        outs[1][...] = stream
        outs[2][...] = normed
    picks = selection(routes_ref[...], first_ref[0], experts, capacity, parcel_ref.shape[0])
    chosen = functools.reduce(jnp.logical_or, picks).astype(F32).astype(BF16)
    parcel_ref[...] = jnp.dot(chosen, normed, preferred_element_type=F32).astype(BF16)


def project(act, weight, residual, gain, routes, first, experts, capacity, rows, keep):
    tokens, width = residual.shape
    out = jax.ShapeDtypeStruct((tokens, width), BF16)
    outs = [jax.ShapeDtypeStruct((rows, width), BF16)] + [out, out] * keep
    smem = pl.BlockSpec(memory_space=pltpu.SMEM)
    vmem = pl.BlockSpec(memory_space=pltpu.VMEM)
    return pl.pallas_call(
        functools.partial(project_body, (experts, capacity), keep),
        out_shape=outs,
        in_specs=[smem] + [vmem] * 5,
        out_specs=[vmem] * len(outs),
        cost_estimate=pl.CostEstimate(
            flops=2 * tokens * weight.size, bytes_accessed=2 * weight.size, transcendentals=0
        ),
        name="project_keep" if keep else "project",
    )(first, act, weight, residual, gain, routes)


def mlp_body(rows_ref, gate_ref, up_ref, down_ref, out_ref, hidden):
    inner = gate_ref.shape[-1]
    width = out_ref.shape[-1]
    rows = rows_ref[...]
    tile = min(inner, 256)
    for n in range(inner // tile):
        cols = pl.ds(n * tile, tile)
        gate = jnp.dot(rows, gate_ref[:, cols], preferred_element_type=F32)
        up = jnp.dot(rows, up_ref[:, cols], preferred_element_type=F32)
        hidden[:, cols] = (jax.nn.silu(gate) * up).astype(BF16)
    tile = min(width, 512)
    for n in range(width // tile):
        cols = pl.ds(n * tile, tile)
        out_ref[:, cols] = jnp.dot(
            hidden[...], down_ref[:, cols], preferred_element_type=F32
        ).astype(out_ref.dtype)


def gated_mlp(rows, gate, up, down, dtype):
    count, width = rows.shape
    inner = gate.shape[-1]
    return call(
        mlp_body,
        jax.ShapeDtypeStruct((count, width), dtype),
        scratch=[pltpu.VMEM((count, inner), BF16)],
        flops=6 * count * width * inner,
        moved=6 * width * inner,
    )(rows, gate, up, down)


def combine_body(shape_of, first_ref, routes_ref, weight_ref, back_ref, *rest):
    experts, capacity = shape_of
    out_ref = rest[-1]
    rows = back_ref.shape[0]
    picks = selection(routes_ref[...], first_ref[0], experts, capacity, rows)
    table = jnp.zeros((rows, routes_ref.shape[1]), F32)
    for k, pick in enumerate(picks):
        table = table + jnp.where(pick, weight_ref[k : k + 1, :], 0.0)
    high = table.astype(BF16)
    low = (table - high.astype(F32)).astype(BF16)
    back = back_ref[...]
    over = (((0,), (0,)), ((), ()))
    total = lax.dot_general(high, back, over, preferred_element_type=F32)
    total = total + lax.dot_general(low, back, over, preferred_element_type=F32)
    for ref in rest[:-1]:
        total = total + ref[...].astype(F32)
    out_ref[...] = total.astype(out_ref.dtype)


def combine(routes, weights, back, first, experts, capacity, dtype, extra):
    rows, width = back.shape
    tokens = routes.shape[1]
    smem = pl.BlockSpec(memory_space=pltpu.SMEM)
    vmem = pl.BlockSpec(memory_space=pltpu.VMEM)
    return pl.pallas_call(
        functools.partial(combine_body, (experts, capacity)),
        out_shape=jax.ShapeDtypeStruct((tokens, width), dtype),
        in_specs=[smem] + [vmem] * (3 + len(extra)),
        out_specs=vmem,
        cost_estimate=pl.CostEstimate(
            flops=4 * tokens * rows * width, bytes_accessed=2 * rows * width, transcendentals=0
        ),
    )(first, routes, weights, back, *extra)


def per_device(
    conv_value,
    conv_gate,
    taps,
    doc_ids,
    gn_gain,
    gn_shift,
    conv_out,
    residual,
    norm_gain,
    routes,
    route_weight,
    expert_gate,
    expert_up,
    expert_down,
    shared_gate,
    shared_up,
    shared_down,
):
    position_count, channel_count = conv_value.shape
    kernel_width = taps.shape[0]
    model_width = residual.shape[1]
    token_count, top_count = routes.shape
    core_split = lax.axis_size("tp")
    half_devices = lax.axis_size("sp") * core_split
    local_experts = expert_gate.shape[0]
    half_experts = local_experts * half_devices
    experts = half_experts * lax.axis_size("half")
    capacity = 2 * token_count * top_count // experts
    half_rows = half_experts * capacity
    first = (lax.axis_index("half").astype(I32) * half_experts).reshape(1)

    mirror_residual = to_mirror(residual)

    rim = -(-(kernel_width - 1) // 8) * 8
    rim_glu = glu_of(conv_value[-rim:], conv_gate[-rim:])
    rim_ids = jnp.broadcast_to(doc_ids[-rim:, None].astype(BF16), (rim, LANES))
    edge = from_behind(jnp.concatenate([rim_glu, rim_ids], axis=1), LINE, 1)
    own_meta = jnp.concatenate([routes.astype(F32), route_weight], axis=1).T
    mirror_meta = to_mirror(own_meta)
    own_routes, own_weight = own_meta[:top_count], own_meta[top_count:]
    mirror_routes, mirror_weight = mirror_meta[:top_count], mirror_meta[top_count:]

    wide_ids = jnp.broadcast_to(doc_ids[:, None].astype(F32), (position_count, LANES))
    conv_act = convolve(
        conv_value,
        conv_gate,
        edge,
        wide_ids,
        taps.astype(F32),
        gn_gain[None, :],
        gn_shift[None, :],
    )
    by_core = conv_act.reshape(core_split, token_count, channel_count)
    act = lax.all_to_all(by_core, "tp", split_axis=0, concat_axis=0, tiled=True)
    mirror_act = to_mirror(act)

    def exchange(rows):
        parcel = rows.reshape(half_devices, local_experts * capacity, model_width)
        arrived = lax.all_to_all(parcel, HALF, split_axis=0, concat_axis=0, tiled=True)
        return arrived.reshape(half_rows, model_width)

    def experts_on(rows):
        split = rows.reshape(half_devices, local_experts, capacity, model_width)
        results = []
        for e in range(local_experts):
            mine = split[:, e].reshape(half_devices * capacity, model_width)
            result = gated_mlp(mine, expert_gate[e], expert_up[e], expert_down[e], BF16)
            results.append(result.reshape(half_devices, capacity, model_width))
        return jnp.stack(results, axis=1)

    sizes = (experts, capacity)
    gain = norm_gain[None, :]
    parcel, stream, normed = project(
        act, conv_out, residual, gain, own_routes, first, *sizes, half_rows, True
    )
    own_arrived = exchange(parcel)
    (mirror_parcel,) = project(
        mirror_act, conv_out, mirror_residual, gain, mirror_routes, first, *sizes, half_rows, False
    )
    mirror_arrived = exchange(mirror_parcel)
    shared_out = gated_mlp(normed, shared_gate, shared_up, shared_down, F32)
    own_result = experts_on(own_arrived)
    mirror_result = experts_on(mirror_arrived)
    mirror_back = exchange(mirror_result)
    partial = combine(mirror_routes, mirror_weight, mirror_back, first, *sizes, BF16, ())
    other_part = to_mirror(partial)
    own_back = exchange(own_result)
    own_part = combine(own_routes, own_weight, own_back, first, *sizes, F32, (stream, shared_out))
    return (own_part + other_part.astype(F32)).astype(BF16)


def solution(mesh):
    sequence_split, core_split = mesh.devices.shape
    folded = Mesh(
        mesh.devices.reshape(2, sequence_split // 2, core_split), ("half", "sp", "tp")
    )
    line, everyone = LINE, LINE + ("tp",)
    return jax.shard_map(
        per_device,
        mesh=folded,
        in_specs=(
            P(line, "tp"),
            P(line, "tp"),
            P(None, "tp"),
            P(line),
            P("tp"),
            P("tp"),
            P(),
            P(everyone, None),
            P(),
            P(everyone, None),
            P(everyone, None),
            P(everyone, None, None),
            P(everyone, None, None),
            P(everyone, None, None),
            P(),
            P(),
            P(),
        ),
        out_specs=P(everyone, None),
        check_vma=False,
    )
```

```python
import functools

import jax
import jax.numpy as jnp
from jax import lax
from jax.experimental import pallas as pl
from jax.experimental.pallas import tpu as pltpu
from jax.sharding import Mesh
from jax.sharding import PartitionSpec as P

LANES = 128


epsilon = 1e-06

HALF = ("sp", "tp")
LINE = ("half", "sp")

F32, BF16, I32 = jnp.float32, jnp.bfloat16, jnp.int32


def from_behind(x, axis, by):
    peers = lax.axis_size(axis)
    pairs = [(i, i + by) for i in range(peers) if 0 <= i + by < peers]
    return lax.ppermute(x, axis, pairs)


def to_mirror(x):
    return lax.ppermute(x, "half", [(0, 1), (1, 0)])


def glu_of(value, gate):
    return (value.astype(F32) * jax.nn.sigmoid(gate.astype(F32))).astype(BF16)


def cost(flops, moved):
    return pl.CostEstimate(
        flops=int(flops), bytes_accessed=int(moved), transcendentals=0
    )


def column_of(row, count, start):
    across = lax.broadcasted_iota(I32, (count, LANES), 1)
    down = lax.broadcasted_iota(I32, (count, LANES), 0)
    picked = jnp.where(across == down + start, row, 0.0)
    return jnp.broadcast_to(jnp.sum(picked, axis=1, keepdims=True), (count, LANES))


def edge_body(value_ref, gate_ref, ids_ref, routes_ref, weight_ref, edge_ref, meta_ref):
    rim, channels = value_ref.shape
    top = routes_ref.shape[0]
    edge_ref[:, pl.ds(0, channels)] = glu_of(value_ref[...], gate_ref[...])
    edge_ref[:, pl.ds(channels, LANES)] = column_of(
        ids_ref[...].astype(F32), rim, LANES - rim
    ).astype(BF16)
    meta_ref[pl.ds(0, top), :] = routes_ref[...].astype(F32)
    meta_ref[pl.ds(top, top), :] = weight_ref[...]


def edge_of(value, gate, ids, routes, weight, rim):
    positions, channels = value.shape
    top, tokens = routes.shape
    tail = pl.BlockSpec((rim, channels), lambda i: (positions // rim - 1, 0))
    whole = pl.BlockSpec((top, tokens), lambda i: (0, 0))
    return pl.pallas_call(
        edge_body,
        grid=(1,),
        out_shape=(
            jax.ShapeDtypeStruct((rim, channels + LANES), BF16),
            jax.ShapeDtypeStruct((2 * top, tokens), F32),
        ),
        in_specs=[
            tail,
            tail,
            pl.BlockSpec((1, LANES), lambda i: (0, positions // LANES - 1)),
            whole,
            whole,
        ],
        out_specs=(
            pl.BlockSpec((rim, channels + LANES), lambda i: (0, 0)),
            pl.BlockSpec((2 * top, tokens), lambda i: (0, 0)),
        ),
        cost_estimate=cost(1e6, 1e5),
        name="edge",
    )(value, gate, ids, routes, weight)


def conv_body(
    core_ref,
    value_ref,
    gate_ref,
    edge_ref,
    ids_ref,
    taps_ref,
    gain_ref,
    shift_ref,
    keep_ref,
    send_ref,
    glu,
    ids,
    weights,
):
    positions, channels = value_ref.shape
    width = taps_ref.shape[0]
    rim = edge_ref.shape[0]
    blocks = channels // LANES
    rows = 32
    tokens = keep_ref.shape[0]
    weights[pl.ds(0, width), :] = taps_ref[...].astype(F32)
    ids[pl.ds(0, rim), :] = edge_ref[:, pl.ds(channels, LANES)].astype(F32)
    for start in range(0, positions, LANES):
        row = ids_ref[:, pl.ds(start, LANES)].astype(F32)
        ids[pl.ds(rim + start, LANES), :] = column_of(row, LANES, 0)
    for c in range(blocks):
        lanes = pl.ds(c * LANES, LANES)
        glu[c, pl.ds(0, rim), :] = edge_ref[:, lanes].astype(F32)
        glu[c, pl.ds(rim, positions), :] = glu_of(value_ref[:, lanes], gate_ref[:, lanes]).astype(
            F32
        )

    def chunk(out_ref, base, index):
        inside = pl.multiple_of(index * rows, rows)
        row = pl.multiple_of(base + inside, rows)
        here = ids[pl.ds(row + rim, rows), :]
        total = [jnp.zeros((rows, LANES), F32) for _ in range(blocks)]
        for tap in range(width):
            past = row + (rim - width + 1 + tap)
            same = ids[pl.ds(past, rows), :] == here
            for c in range(blocks):
                weight = weights[pl.ds(tap, 1), pl.ds(c * LANES, LANES)]
                term = weight * glu[c, pl.ds(past, rows), :]
                total[c] = total[c] + jnp.where(same, term, 0.0)
        for c in range(blocks):
            lanes = pl.ds(c * LANES, LANES)
            centered = total[c] - jnp.mean(total[c], axis=-1, keepdims=True)
            spread = jnp.mean(centered * centered, axis=-1, keepdims=True)
            scaled = centered * lax.rsqrt(spread + epsilon)
            out_ref[pl.ds(inside, rows), lanes] = jax.nn.silu(
                scaled * gain_ref[:, lanes] + shift_ref[:, lanes]
            ).astype(BF16)

    core = core_ref[0]
    parts = positions // tokens
    for out_ref, part in ((send_ref, parts - 1 - core), (keep_ref, core)):
        base = pl.multiple_of(part * tokens, tokens)

        def step(index, carry, out_ref=out_ref, base=base):
            chunk(out_ref, base, index)
            return carry

        lax.fori_loop(0, tokens // rows, step, 0)


def convolve(core, value, gate, edge, ids, taps, gain, shift, tokens):
    positions, channels = value.shape
    rim = edge.shape[0]
    half = jax.ShapeDtypeStruct((tokens, channels), BF16)
    return pl.pallas_call(
        conv_body,
        out_shape=(half, half),
        in_specs=[pl.BlockSpec(memory_space=pltpu.SMEM)]
        + [pl.BlockSpec(memory_space=pltpu.VMEM)] * 7,
        scratch_shapes=[
            pltpu.VMEM((channels // LANES, rim + positions, LANES), F32),
            pltpu.VMEM((rim + positions, LANES), F32),
            pltpu.VMEM((-(-taps.shape[0] // 8) * 8, channels), F32),
        ],
        cost_estimate=cost(6e9, 6 * value.size),
        name="conv",
    )(core, value, gate, edge, ids, taps, gain, shift)


def selection(routes, first, experts, capacity, rows):
    top, tokens = routes.shape
    routes = routes.astype(I32)
    names = lax.broadcasted_iota(I32, (experts, tokens), 0)
    earlier = lax.broadcasted_iota(I32, (tokens, tokens), 0) < lax.broadcasted_iota(
        I32, (tokens, tokens), 1
    )
    earlier = earlier.astype(F32).astype(BF16)
    index = lax.broadcasted_iota(I32, (rows, tokens), 0)
    used = jnp.zeros((experts, 1), F32)
    picks = []
    for k in range(top):
        route = routes[k : k + 1, :]
        chosen = (names == route).astype(F32)
        before = jnp.dot(chosen.astype(BF16), earlier, preferred_element_type=F32) + used
        slot = jnp.sum(chosen * before, axis=0, keepdims=True).astype(I32)
        picks.append(index == (route - first) * capacity + slot)
        used = used + jnp.sum(chosen, axis=1, keepdims=True)
    return picks


def chosen_of(picks):
    return functools.reduce(jnp.logical_or, picks).astype(F32).astype(BF16)


def project_body(
    shape_of,
    first_ref,
    core_ref,
    keep_ref,
    got_ref,
    weight_hbm,
    residual_ref,
    gain_ref,
    meta_ref,
    parcel_ref,
    stream_ref,
    normed_ref,
    weight,
    total,
    sems,
):
    experts, capacity, top = shape_of
    depth = keep_ref.shape[1]
    chunks = weight.shape[0]
    step = weight.shape[1]
    core = core_ref[0]
    copies = []
    for index in range(chunks):
        part, inside = divmod(index * step, depth)
        owner = core if part == 0 else 1 - core
        start = pl.multiple_of(owner * depth + inside, step)
        copy = pltpu.make_async_copy(
            weight_hbm.at[pl.ds(start, step), :], weight.at[index], sems.at[index]
        )
        copy.start()
        copies.append(copy)
    picks = selection(
        meta_ref[pl.ds(0, top), :], first_ref[0], experts, capacity, parcel_ref.shape[0]
    )
    chosen = chosen_of(picks)
    total[...] = residual_ref[...].astype(F32)
    for index, copy in enumerate(copies):
        part, inside = divmod(index * step, depth)
        act = (keep_ref if part == 0 else got_ref)[:, pl.ds(inside, step)]
        copy.wait()
        total[...] += jnp.dot(act, weight[index], preferred_element_type=F32)
    stream = total[...].astype(BF16)
    wide = stream.astype(F32)
    normed = (
        wide * lax.rsqrt(jnp.mean(wide * wide, axis=-1, keepdims=True) + epsilon) * gain_ref[...]
    ).astype(BF16)
    stream_ref[...] = stream
    normed_ref[...] = normed
    parcel_ref[...] = jnp.dot(chosen, normed, preferred_element_type=F32).astype(BF16)


def project(first, core, keep, got, weight, residual, gain, meta, sizes, rows):
    tokens, width = residual.shape
    depth = keep.shape[1]
    step = depth // 2
    chunks = 2 * depth // step
    out = jax.ShapeDtypeStruct((tokens, width), BF16)
    smem = pl.BlockSpec(memory_space=pltpu.SMEM)
    vmem = pl.BlockSpec(memory_space=pltpu.VMEM)
    return pl.pallas_call(
        functools.partial(project_body, sizes),
        out_shape=(jax.ShapeDtypeStruct((rows, width), BF16), out, out),
        in_specs=[smem, smem, vmem, vmem, pl.BlockSpec(memory_space=pl.ANY), vmem, vmem, vmem],
        out_specs=[vmem] * 3,
        scratch_shapes=[
            pltpu.VMEM((chunks, step, width), BF16),
            pltpu.VMEM((tokens, width), F32),
            pltpu.SemaphoreType.DMA((chunks,)),
        ],
        cost_estimate=cost(2 * tokens * weight.size, 2 * weight.size),
        name="project",
    )(first, core, keep, got, weight, residual, gain, meta)


def gather_body(shape_of, first_ref, meta_ref, rows_ref, parcel_ref, chosen):
    experts, capacity, top = shape_of

    @pl.when(pl.program_id(0) == 0)
    def _():
        picks = selection(
            meta_ref[pl.ds(0, top), :], first_ref[0], experts, capacity, parcel_ref.shape[0]
        )
        chosen[...] = chosen_of(picks)

    parcel_ref[...] = jnp.dot(chosen[...], rows_ref[...], preferred_element_type=F32).astype(BF16)


def gather(first, meta, rows, sizes, count):
    tokens, width = rows.shape
    tile = width // 2
    return pl.pallas_call(
        functools.partial(gather_body, sizes),
        grid=(width // tile,),
        out_shape=jax.ShapeDtypeStruct((count, width), BF16),
        in_specs=[
            pl.BlockSpec(memory_space=pltpu.SMEM),
            pl.BlockSpec(meta.shape, lambda n: (0, 0)),
            pl.BlockSpec((tokens, tile), lambda n: (0, n)),
        ],
        out_specs=pl.BlockSpec((count, tile), lambda n: (0, n)),
        scratch_shapes=[pltpu.VMEM((count, tokens), BF16)],
        cost_estimate=cost(2 * count * tokens * width, 2 * (count + tokens) * width),
        name="gather",
    )(first, meta, rows)


def mlp_body(
    steps,
    rows_hbm,
    gate_hbm,
    up_hbm,
    down_hbm,
    *rest,
):
    extra = rest[:-11]
    (out_hbm, rows, gate, up, down, total_gate, total_up, hidden, out, in_sems, out_sems) = rest[
        -11:
    ]
    depth = gate.shape[0] // steps
    tile = down.shape[1] // steps
    rows_copy = pltpu.make_async_copy(rows_hbm, rows, in_sems.at[0])
    rows_copy.start()
    wide, narrow = [], []
    for n in range(steps):
        part = pl.ds(n * depth, depth)
        pair = (
            pltpu.make_async_copy(gate_hbm.at[part, :], gate.at[part, :], in_sems.at[1 + 3 * n]),
            pltpu.make_async_copy(up_hbm.at[part, :], up.at[part, :], in_sems.at[2 + 3 * n]),
        )
        for copy in pair:
            copy.start()
        wide.append(pair)
    for n in range(steps):
        cols = pl.ds(n * tile, tile)
        copy = pltpu.make_async_copy(down_hbm.at[:, cols], down.at[:, cols], in_sems.at[3 + 3 * n])
        copy.start()
        narrow.append(copy)
    rows_copy.wait()
    for n, pair in enumerate(wide):
        part = pl.ds(n * depth, depth)
        for copy, weight, total in zip(pair, (gate, up), (total_gate, total_up)):
            copy.wait()
            product = jnp.dot(rows[:, part], weight[part, :], preferred_element_type=F32)
            total[...] = product if n == 0 else total[...] + product
    hidden[...] = (jax.nn.silu(total_gate[...]) * total_up[...]).astype(BF16)
    back = []
    for n, copy in enumerate(narrow):
        cols = pl.ds(n * tile, tile)
        copy.wait()
        result = jnp.dot(hidden[...], down[:, cols], preferred_element_type=F32)
        for ref in extra:
            result = result + ref[:, cols].astype(F32)
        out[:, cols] = result.astype(out.dtype)
        copy = pltpu.make_async_copy(out.at[:, cols], out_hbm.at[:, cols], out_sems.at[n])
        copy.start()
        back.append(copy)
    for copy in back:
        copy.wait()


def gated_mlp(rows, gate, up, down, extra, dtype):
    count, width = rows.shape
    inner = gate.shape[-1]
    steps = 4
    anywhere = pl.BlockSpec(memory_space=pl.ANY)
    return pl.pallas_call(
        functools.partial(mlp_body, steps),
        out_shape=jax.ShapeDtypeStruct((count, width), dtype),
        in_specs=[anywhere] * 4 + [pl.BlockSpec(memory_space=pltpu.VMEM)] * len(extra),
        out_specs=anywhere,
        scratch_shapes=[
            pltpu.VMEM((count, width), rows.dtype),
            pltpu.VMEM((width, inner), gate.dtype),
            pltpu.VMEM((width, inner), up.dtype),
            pltpu.VMEM((inner, width), down.dtype),
            pltpu.VMEM((count, inner), F32),
            pltpu.VMEM((count, inner), F32),
            pltpu.VMEM((count, inner), BF16),
            pltpu.VMEM((count, width), dtype),
            pltpu.SemaphoreType.DMA((1 + 3 * steps,)),
            pltpu.SemaphoreType.DMA((steps,)),
        ],
        cost_estimate=cost(6 * count * width * inner, 6 * width * inner),
    )(rows, gate, up, down, *extra)


def combine_body(shape_of, first_ref, meta_ref, back_ref, *rest):
    experts, capacity, top = shape_of
    out_ref, high, low = rest[-3:]

    @pl.when(pl.program_id(0) == 0)
    def _():
        rows = back_ref.shape[0]
        picks = selection(meta_ref[pl.ds(0, top), :], first_ref[0], experts, capacity, rows)
        table = jnp.zeros((rows, meta_ref.shape[1]), F32)
        for k, pick in enumerate(picks):
            table = table + jnp.where(pick, meta_ref[pl.ds(top + k, 1), :], 0.0)
        table = table.T
        high[...] = table.astype(BF16)
        low[...] = (table - table.astype(BF16).astype(F32)).astype(BF16)

    back = back_ref[...]
    total = jnp.dot(high[...], back, preferred_element_type=F32)
    total = total + jnp.dot(low[...], back, preferred_element_type=F32)
    for ref in rest[:-3]:
        total = total + ref[...].astype(F32)
    out_ref[...] = total.astype(out_ref.dtype)


def combine(first, meta, back, sizes, extra):
    rows, width = back.shape
    tokens = meta.shape[1]
    tile = width // 2
    row = pl.BlockSpec((tokens, tile), lambda n: (0, n))
    return pl.pallas_call(
        functools.partial(combine_body, sizes),
        grid=(width // tile,),
        out_shape=jax.ShapeDtypeStruct((tokens, width), BF16),
        in_specs=[
            pl.BlockSpec(memory_space=pltpu.SMEM),
            pl.BlockSpec(meta.shape, lambda n: (0, 0)),
            pl.BlockSpec((rows, tile), lambda n: (0, n)),
        ]
        + [row] * len(extra),
        out_specs=row,
        scratch_shapes=[pltpu.VMEM((tokens, rows), BF16)] * 2,
        cost_estimate=cost(4 * tokens * rows * width, 2 * rows * width),
    )(first, meta, back, *extra)


def per_device(
    conv_value,
    conv_gate,
    taps,
    doc_ids,
    gn_gain,
    gn_shift,
    conv_out,
    residual,
    norm_gain,
    routes,
    route_weight,
    expert_gate,
    expert_up,
    expert_down,
    shared_gate,
    shared_up,
    shared_down,
):
    kernel_width = taps.shape[0]
    model_width = residual.shape[1]
    token_count, top_count = routes.shape
    half_devices = lax.axis_size("sp") * lax.axis_size("tp")
    local_experts = expert_gate.shape[0]
    half_experts = local_experts * half_devices
    experts = half_experts * lax.axis_size("half")
    capacity = 2 * token_count * top_count // experts
    half_rows = half_experts * capacity
    first = (lax.axis_index("half").astype(I32) * half_experts).reshape(1)
    core = lax.axis_index("tp").astype(I32).reshape(1)
    sizes = (experts, capacity, top_count)

    rim = -(-(kernel_width - 1) // 16) * 16
    ids = doc_ids[None, :]
    own_edge, own_meta = edge_of(conv_value, conv_gate, ids, routes.T, route_weight.T, rim)
    edge = from_behind(own_edge, LINE, 1)
    mirror_meta = to_mirror(own_meta)
    keep, send = convolve(
        core,
        conv_value,
        conv_gate,
        edge,
        ids,
        taps,
        gn_gain[None, :],
        gn_shift[None, :],
        token_count,
    )
    got = lax.ppermute(send, "tp", [(0, 1), (1, 0)])
    parcel, stream, normed = project(
        first, core, keep, got, conv_out, residual, norm_gain[None, :], own_meta, sizes, half_rows
    )
    mirror_normed = to_mirror(normed)

    def exchange(rows):
        parcel = rows.reshape(half_devices, local_experts * capacity, model_width)
        arrived = lax.all_to_all(parcel, HALF, split_axis=0, concat_axis=0, tiled=True)
        return arrived.reshape(half_rows, model_width)

    def experts_on(rows):
        split = rows.reshape(half_devices, local_experts, capacity, model_width)
        results = []
        for e in range(local_experts):
            mine = split[:, e].reshape(half_devices * capacity, model_width)
            result = gated_mlp(mine, expert_gate[e], expert_up[e], expert_down[e], (), BF16)
            results.append(result.reshape(half_devices, capacity, model_width))
        return jnp.stack(results, axis=1)

    own_arrived = exchange(parcel)
    mirror_parcel = gather(first, mirror_meta, mirror_normed, sizes, half_rows)
    mirror_arrived = exchange(mirror_parcel)
    base = gated_mlp(normed, shared_gate, shared_up, shared_down, (stream,), F32)
    own_result = experts_on(own_arrived)
    mirror_result = experts_on(mirror_arrived)
    mirror_back = exchange(mirror_result)
    partial = combine(first, mirror_meta, mirror_back, sizes, ())
    other_part = to_mirror(partial)
    own_back = exchange(own_result)
    return combine(first, own_meta, own_back, sizes, (base, other_part))


def solution(mesh):
    sequence_split, core_split = mesh.devices.shape
    folded = Mesh(
        mesh.devices.reshape(2, sequence_split // 2, core_split), ("half", "sp", "tp")
    )
    line, everyone = LINE, LINE + ("tp",)
    return jax.shard_map(
        per_device,
        mesh=folded,
        in_specs=(
            P(line, "tp"),
            P(line, "tp"),
            P(None, "tp"),
            P(line),
            P("tp"),
            P("tp"),
            P(),
            P(everyone, None),
            P(),
            P(everyone, None),
            P(everyone, None),
            P(everyone, None, None),
            P(everyone, None, None),
            P(everyone, None, None),
            P(),
            P(),
            P(),
        ),
        out_specs=P(everyone, None),
        check_vma=False,
    )
```

```python
import functools

import jax
import jax.numpy as jnp
from jax import lax
from jax.experimental import pallas as pl
from jax.experimental.pallas import tpu as pltpu
from jax.sharding import Mesh
from jax.sharding import PartitionSpec as P

LANES = 128


epsilon = 1e-06

HALF = ("sp", "tp")
LINE = ("half", "sp")

F32, BF16, I32 = jnp.float32, jnp.bfloat16, jnp.int32

ROWS = 32
STEPS = 4

SMEM = pl.BlockSpec(memory_space=pltpu.SMEM)
VMEM = pl.BlockSpec(memory_space=pltpu.VMEM)
ANY = pl.BlockSpec(memory_space=pl.ANY)
PARAMS = pltpu.CompilerParams(vmem_limit_bytes=24 * 2**20)


def from_behind(x, axis, by):
    peers = lax.axis_size(axis)
    pairs = [(i, i + by) for i in range(peers) if 0 <= i + by < peers]
    return lax.ppermute(x, axis, pairs)


def to_mirror(x):
    return lax.ppermute(x, "half", [(0, 1), (1, 0)])


def glu_of(value, gate):
    return (value.astype(F32) * jax.nn.sigmoid(gate.astype(F32))).astype(BF16)


def cost(flops, moved):
    return pl.CostEstimate(
        flops=int(flops), bytes_accessed=int(moved), transcendentals=0
    )


def column_of(row, count, start):
    across = lax.broadcasted_iota(I32, (count, LANES), 1)
    down = lax.broadcasted_iota(I32, (count, LANES), 0)
    picked = jnp.where(across == down + start, row, 0.0)
    return jnp.broadcast_to(jnp.sum(picked, axis=1, keepdims=True), (count, LANES))


def edge_body(value_ref, gate_ref, ids_ref, routes_ref, weight_ref, edge_ref, meta_ref):
    rim, channels = value_ref.shape
    top = routes_ref.shape[0]
    edge_ref[:, pl.ds(0, channels)] = glu_of(value_ref[...], gate_ref[...])
    edge_ref[:, pl.ds(channels, LANES)] = column_of(
        ids_ref[...].astype(F32), rim, LANES - rim
    ).astype(BF16)
    meta_ref[pl.ds(0, top), :] = routes_ref[...].astype(F32)
    meta_ref[pl.ds(top, top), :] = weight_ref[...]


def edge_of(value, gate, ids, routes, weight, rim):
    positions, channels = value.shape
    top, tokens = routes.shape
    tail = pl.BlockSpec((rim, channels), lambda i: (positions // rim - 1, 0))
    whole = pl.BlockSpec((top, tokens), lambda i: (0, 0))
    return pl.pallas_call(
        edge_body,
        grid=(1,),
        out_shape=(
            jax.ShapeDtypeStruct((rim, channels + LANES), BF16),
            jax.ShapeDtypeStruct((2 * top, tokens), F32),
        ),
        in_specs=[
            tail,
            tail,
            pl.BlockSpec((1, LANES), lambda i: (0, positions // LANES - 1)),
            whole,
            whole,
        ],
        out_specs=(
            pl.BlockSpec((rim, channels + LANES), lambda i: (0, 0)),
            pl.BlockSpec((2 * top, tokens), lambda i: (0, 0)),
        ),
        cost_estimate=cost(1e6, 1e5),
        compiler_params=PARAMS,
        name="edge",
    )(value, gate, ids, routes, weight)


def conv_rows(row, count, rim, width, blocks, glu, ids, weights, gain_ref, shift_ref, store):
    here = ids[pl.ds(row + rim, count), :]
    total = [jnp.zeros((count, LANES), F32) for _ in range(blocks)]
    for tap in range(width):
        past = row + (rim - width + 1 + tap)
        same = ids[pl.ds(past, count), :] == here
        for c in range(blocks):
            weight = weights[pl.ds(tap, 1), pl.ds(c * LANES, LANES)]
            term = weight * glu[c, pl.ds(past, count), :]
            total[c] = total[c] + jnp.where(same, term, 0.0)
    for c in range(blocks):
        lanes = pl.ds(c * LANES, LANES)
        centered = total[c] - jnp.mean(total[c], axis=-1, keepdims=True)
        spread = jnp.mean(centered * centered, axis=-1, keepdims=True)
        scaled = centered * lax.rsqrt(spread + epsilon)
        store(
            lanes,
            jax.nn.silu(scaled * gain_ref[:, lanes] + shift_ref[:, lanes]).astype(BF16),
        )


def conv_body(
    core_ref,
    value_ref,
    gate_ref,
    ids_ref,
    taps_ref,
    gain_ref,
    shift_ref,
    keep_ref,
    send_ref,
    glu,
    ids,
    weights,
):
    positions, channels = value_ref.shape
    width = taps_ref.shape[0]
    blocks = channels // LANES
    rows = ROWS
    tokens = keep_ref.shape[0]
    weights[pl.ds(0, width), :] = taps_ref[...].astype(F32)
    for start in range(0, positions, LANES):
        row = ids_ref[:, pl.ds(start, LANES)].astype(F32)
        ids[pl.ds(start, LANES), :] = column_of(row, LANES, 0)
    for c in range(blocks):
        lanes = pl.ds(c * LANES, LANES)
        glu[c] = glu_of(value_ref[:, lanes], gate_ref[:, lanes]).astype(F32)

    core = core_ref[0]
    parts = positions // tokens
    for out_ref, part in ((send_ref, parts - 1 - core), (keep_ref, core)):

        def step(index, carry, out_ref=out_ref, part=part):
            inside = pl.multiple_of(index * rows, rows)
            row = pl.multiple_of(part * tokens + inside - rows, rows)

            def store(lanes, act):
                out_ref[pl.ds(inside, rows), lanes] = act

            conv_rows(
                row, rows, rows, width, blocks, glu, ids, weights, gain_ref, shift_ref, store
            )
            return carry

        lax.fori_loop((part == 0).astype(I32), tokens // rows, step, 0)


def convolve(core, value, gate, ids, taps, gain, shift, tokens):
    positions, channels = value.shape
    half = jax.ShapeDtypeStruct((tokens, channels), BF16)
    return pl.pallas_call(
        conv_body,
        out_shape=(half, half),
        in_specs=[SMEM] + [VMEM] * 6,
        scratch_shapes=[
            pltpu.VMEM((channels // LANES, positions, LANES), F32),
            pltpu.VMEM((positions, LANES), F32),
            pltpu.VMEM((-(-taps.shape[0] // 8) * 8, channels), F32),
        ],
        cost_estimate=cost(6e9, 6 * value.size),
        compiler_params=PARAMS,
        name="conv",
    )(core, value, gate, ids, taps, gain, shift)


def rim_body(
    core_ref,
    edge_hbm,
    value_ref,
    gate_ref,
    ids_ref,
    taps_ref,
    gain_ref,
    shift_ref,
    keep_in,
    send_in,
    keep_hbm,
    send_hbm,
    edge,
    glu,
    ids,
    weights,
    act,
    sems,
):
    rows, channels = value_ref.shape
    width = taps_ref.shape[0]
    blocks = channels // LANES
    arrival = pltpu.make_async_copy(edge_hbm, edge, sems.at[0])
    arrival.start()
    weights[pl.ds(0, width), :] = taps_ref[...].astype(F32)
    ids[pl.ds(rows, rows), :] = column_of(ids_ref[...].astype(F32), rows, 0)
    for c in range(blocks):
        lanes = pl.ds(c * LANES, LANES)
        glu[c, pl.ds(rows, rows), :] = glu_of(value_ref[:, lanes], gate_ref[:, lanes]).astype(F32)
    arrival.wait()
    ids[pl.ds(0, rows), :] = edge[:, pl.ds(channels, LANES)].astype(F32)
    for c in range(blocks):
        glu[c, pl.ds(0, rows), :] = edge[:, pl.ds(c * LANES, LANES)].astype(F32)

    def store(lanes, value):
        act[:, lanes] = value

    conv_rows(0, rows, rows, width, blocks, glu, ids, weights, gain_ref, shift_ref, store)

    for mine, out_hbm in ((core_ref[0] == 0, keep_hbm), (core_ref[0] != 0, send_hbm)):

        @pl.when(mine)
        def _(out_hbm=out_hbm):
            copy = pltpu.make_async_copy(act, out_hbm.at[pl.ds(0, rows), :], sems.at[1])
            copy.start()
            copy.wait()


def convolve_rim(core, edge, value, gate, ids, taps, gain, shift, keep, send):
    channels = value.shape[1]
    head = pl.BlockSpec((ROWS, channels), lambda i: (0, 0))

    def whole(x):
        return pl.BlockSpec(x.shape, lambda i: (0, 0))

    return pl.pallas_call(
        rim_body,
        grid=(1,),
        out_shape=(
            jax.ShapeDtypeStruct(keep.shape, BF16),
            jax.ShapeDtypeStruct(send.shape, BF16),
        ),
        in_specs=[
            SMEM,
            ANY,
            head,
            head,
            pl.BlockSpec((1, LANES), lambda i: (0, 0)),
            whole(taps),
            whole(gain),
            whole(shift),
            ANY,
            ANY,
        ],
        out_specs=(ANY, ANY),
        input_output_aliases={8: 0, 9: 1},
        scratch_shapes=[
            pltpu.VMEM(edge.shape, BF16),
            pltpu.VMEM((channels // LANES, 2 * ROWS, LANES), F32),
            pltpu.VMEM((2 * ROWS, LANES), F32),
            pltpu.VMEM((-(-taps.shape[0] // 8) * 8, channels), F32),
            pltpu.VMEM((ROWS, channels), BF16),
            pltpu.SemaphoreType.DMA((2,)),
        ],
        cost_estimate=cost(1e9, 4e5),
        compiler_params=PARAMS,
        name="rim",
    )(core, edge, value, gate, ids, taps, gain, shift, keep, send)


def selection(routes, first, experts, capacity, rows):
    top, tokens = routes.shape
    routes = routes.astype(I32)
    names = lax.broadcasted_iota(I32, (experts, tokens), 0)
    earlier = lax.broadcasted_iota(I32, (tokens, tokens), 0) < lax.broadcasted_iota(
        I32, (tokens, tokens), 1
    )
    earlier = earlier.astype(F32).astype(BF16)
    index = lax.broadcasted_iota(I32, (rows, tokens), 0)
    used = jnp.zeros((experts, 1), F32)
    picks = []
    for k in range(top):
        route = routes[k : k + 1, :]
        chosen = (names == route).astype(F32)
        before = jnp.dot(chosen.astype(BF16), earlier, preferred_element_type=F32) + used
        slot = jnp.sum(chosen * before, axis=0, keepdims=True).astype(I32)
        picks.append(index == (route - first) * capacity + slot)
        used = used + jnp.sum(chosen, axis=1, keepdims=True)
    return picks


def chosen_of(picks):
    return functools.reduce(jnp.logical_or, picks).astype(F32).astype(BF16)


def project_body(
    shape_of,
    first_ref,
    core_ref,
    meta_ref,
    gain_ref,
    keep_hbm,
    got_hbm,
    weight_hbm,
    residual_hbm,
    parcel_hbm,
    stream_hbm,
    normed_hbm,
    act,
    weight,
    total,
    residual,
    stream,
    normed,
    parcel,
    act_sems,
    in_sems,
    out_sems,
):
    experts, capacity, top = shape_of
    depth = keep_hbm.shape[1]
    chunks, step, width = weight.shape
    core = core_ref[0]
    arrivals = []
    for index, source in enumerate((keep_hbm, got_hbm)):
        copy = pltpu.make_async_copy(source, act.at[index], act_sems.at[index])
        copy.start()
        arrivals.append(copy)
    copies = []
    for index in range(chunks):
        part, inside = divmod(index * step, depth)
        owner = core if part == 0 else 1 - core
        start = pl.multiple_of(owner * depth + inside, step)
        copy = pltpu.make_async_copy(
            weight_hbm.at[pl.ds(start, step), :], weight.at[index], in_sems.at[index]
        )
        copy.start()
        copies.append(copy)
    old = pltpu.make_async_copy(residual_hbm, residual, act_sems.at[2])
    old.start()
    picks = selection(
        meta_ref[pl.ds(0, top), :], first_ref[0], experts, capacity, parcel.shape[0]
    )
    chosen = chosen_of(picks)
    for index, copy in enumerate(copies):
        part, inside = divmod(index * step, depth)
        if inside == 0:
            arrivals[part].wait()
        copy.wait()
        product = jnp.dot(
            act[part, :, pl.ds(inside, step)], weight[index], preferred_element_type=F32
        )
        if index == 0:
            total[...] = product
        else:
            total[...] += product
    old.wait()
    stream[...] = (residual[...].astype(F32) + total[...]).astype(BF16)
    back = [pltpu.make_async_copy(stream, stream_hbm, out_sems.at[0])]
    back[0].start()
    wide = stream[...].astype(F32)
    normed[...] = (
        wide * lax.rsqrt(jnp.mean(wide * wide, axis=-1, keepdims=True) + epsilon) * gain_ref[...]
    ).astype(BF16)
    back.append(pltpu.make_async_copy(normed, normed_hbm, out_sems.at[1]))
    back[1].start()
    tile = width // STEPS
    for n in range(STEPS):
        cols = pl.ds(n * tile, tile)
        parcel[:, cols] = jnp.dot(chosen, normed[:, cols], preferred_element_type=F32).astype(BF16)
        copy = pltpu.make_async_copy(
            parcel.at[:, cols], parcel_hbm.at[:, cols], out_sems.at[2 + n]
        )
        copy.start()
        back.append(copy)
    for copy in back:
        copy.wait()


def project(first, core, keep, got, weight, residual, gain, meta, sizes, rows):
    tokens, width = residual.shape
    depth = keep.shape[1]
    step = depth // 2
    chunks = 2 * depth // step
    out = jax.ShapeDtypeStruct((tokens, width), BF16)
    return pl.pallas_call(
        functools.partial(project_body, sizes),
        out_shape=(jax.ShapeDtypeStruct((rows, width), BF16), out, out),
        in_specs=[SMEM, SMEM, VMEM, VMEM] + [ANY] * 4,
        out_specs=[ANY] * 3,
        scratch_shapes=[
            pltpu.VMEM((2, tokens, depth), BF16),
            pltpu.VMEM((chunks, step, width), BF16),
            pltpu.VMEM((tokens, width), F32),
            pltpu.VMEM((tokens, width), BF16),
            pltpu.VMEM((tokens, width), BF16),
            pltpu.VMEM((tokens, width), BF16),
            pltpu.VMEM((rows, width), BF16),
            pltpu.SemaphoreType.DMA((3,)),
            pltpu.SemaphoreType.DMA((chunks,)),
            pltpu.SemaphoreType.DMA((2 + STEPS,)),
        ],
        cost_estimate=cost(2 * tokens * weight.size, 2 * weight.size),
        compiler_params=PARAMS,
        name="project",
    )(first, core, meta, gain, keep, got, weight, residual)


def stream_in(source, target, sems):
    tile = target.shape[1] // STEPS
    copies = []
    for n in range(STEPS):
        cols = pl.ds(n * tile, tile)
        copies.append(pltpu.make_async_copy(source.at[:, cols], target.at[:, cols], sems.at[n]))
        copies[-1].start()
    return copies


def gather_body(
    shape_of, first_ref, meta_ref, rows_hbm, parcel_hbm, rows, parcel, in_sems, out_sems
):
    experts, capacity, top = shape_of
    copies = stream_in(rows_hbm, rows, in_sems)
    picks = selection(
        meta_ref[pl.ds(0, top), :], first_ref[0], experts, capacity, parcel.shape[0]
    )
    chosen = chosen_of(picks)
    tile = rows.shape[1] // STEPS
    back = []
    for n, copy in enumerate(copies):
        cols = pl.ds(n * tile, tile)
        copy.wait()
        parcel[:, cols] = jnp.dot(chosen, rows[:, cols], preferred_element_type=F32).astype(BF16)
        back.append(
            pltpu.make_async_copy(parcel.at[:, cols], parcel_hbm.at[:, cols], out_sems.at[n])
        )
        back[-1].start()
    for copy in back:
        copy.wait()


def gather(first, meta, rows, sizes, count):
    tokens, width = rows.shape
    return pl.pallas_call(
        functools.partial(gather_body, sizes),
        out_shape=jax.ShapeDtypeStruct((count, width), BF16),
        in_specs=[SMEM, VMEM, ANY],
        out_specs=ANY,
        scratch_shapes=[
            pltpu.VMEM((tokens, width), BF16),
            pltpu.VMEM((count, width), BF16),
            pltpu.SemaphoreType.DMA((STEPS,)),
            pltpu.SemaphoreType.DMA((STEPS,)),
        ],
        cost_estimate=cost(2 * count * tokens * width, 2 * (count + tokens) * width),
        compiler_params=PARAMS,
        name="gather",
    )(first, meta, rows)


def mlp_body(
    steps,
    rows_hbm,
    gate_hbm,
    up_hbm,
    down_hbm,
    *rest,
):
    extra = rest[:-11]
    (out_hbm, rows, gate, up, down, total_gate, total_up, hidden, out, in_sems, out_sems) = rest[
        -11:
    ]
    depth = gate.shape[0] // steps
    tile = down.shape[1] // steps
    rows_copy = pltpu.make_async_copy(rows_hbm, rows, in_sems.at[0])
    rows_copy.start()
    wide, narrow = [], []
    for n in range(steps):
        part = pl.ds(n * depth, depth)
        pair = (
            pltpu.make_async_copy(gate_hbm.at[part, :], gate.at[part, :], in_sems.at[1 + 3 * n]),
            pltpu.make_async_copy(up_hbm.at[part, :], up.at[part, :], in_sems.at[2 + 3 * n]),
        )
        for copy in pair:
            copy.start()
        wide.append(pair)
    for n in range(steps):
        cols = pl.ds(n * tile, tile)
        copy = pltpu.make_async_copy(down_hbm.at[:, cols], down.at[:, cols], in_sems.at[3 + 3 * n])
        copy.start()
        narrow.append(copy)
    rows_copy.wait()
    for n, pair in enumerate(wide):
        part = pl.ds(n * depth, depth)
        for copy, weight, total in zip(pair, (gate, up), (total_gate, total_up)):
            copy.wait()
            product = jnp.dot(rows[:, part], weight[part, :], preferred_element_type=F32)
            total[...] = product if n == 0 else total[...] + product
    hidden[...] = (jax.nn.silu(total_gate[...]) * total_up[...]).astype(BF16)
    back = []
    for n, copy in enumerate(narrow):
        cols = pl.ds(n * tile, tile)
        copy.wait()
        result = jnp.dot(hidden[...], down[:, cols], preferred_element_type=F32)
        for ref in extra:
            result = result + ref[:, cols].astype(F32)
        out[:, cols] = result.astype(out.dtype)
        copy = pltpu.make_async_copy(out.at[:, cols], out_hbm.at[:, cols], out_sems.at[n])
        copy.start()
        back.append(copy)
    for copy in back:
        copy.wait()


def gated_mlp(rows, gate, up, down, extra, dtype):
    count, width = rows.shape
    inner = gate.shape[-1]
    steps = STEPS
    return pl.pallas_call(
        functools.partial(mlp_body, steps),
        out_shape=jax.ShapeDtypeStruct((count, width), dtype),
        in_specs=[ANY] * 4 + [VMEM] * len(extra),
        out_specs=ANY,
        scratch_shapes=[
            pltpu.VMEM((count, width), rows.dtype),
            pltpu.VMEM((width, inner), gate.dtype),
            pltpu.VMEM((width, inner), up.dtype),
            pltpu.VMEM((inner, width), down.dtype),
            pltpu.VMEM((count, inner), F32),
            pltpu.VMEM((count, inner), F32),
            pltpu.VMEM((count, inner), BF16),
            pltpu.VMEM((count, width), dtype),
            pltpu.SemaphoreType.DMA((1 + 3 * steps,)),
            pltpu.SemaphoreType.DMA((steps,)),
        ],
        cost_estimate=cost(6 * count * width * inner, 6 * width * inner),
        compiler_params=PARAMS,
    )(rows, gate, up, down, *extra)


def combine_body(shape_of, extras, first_ref, meta_ref, back_hbm, *rest):
    experts, capacity, top = shape_of
    extra_hbm, rest = rest[:extras], rest[extras:]
    out_hbm, rest = rest[0], rest[1:]
    extra, rest = rest[:extras], rest[extras:]
    back, out, in_sems, out_sems = rest
    rows = back.shape[0]
    arrivals = [stream_in(back_hbm, back, in_sems.at[0])]
    for index in range(extras):
        arrivals.append(stream_in(extra_hbm[index], extra[index], in_sems.at[1 + index]))
    picks = selection(meta_ref[pl.ds(0, top), :], first_ref[0], experts, capacity, rows)
    table = jnp.zeros((rows, meta_ref.shape[1]), F32)
    for k, pick in enumerate(picks):
        table = table + jnp.where(pick, meta_ref[pl.ds(top + k, 1), :], 0.0)
    table = table.T
    high = table.astype(BF16)
    low = (table - high.astype(F32)).astype(BF16)
    tile = back.shape[1] // STEPS
    done = []
    for n in range(STEPS):
        cols = pl.ds(n * tile, tile)
        for copies in arrivals:
            copies[n].wait()
        total = jnp.dot(high, back[:, cols], preferred_element_type=F32)
        total = total + jnp.dot(low, back[:, cols], preferred_element_type=F32)
        for ref in extra:
            total = total + ref[:, cols].astype(F32)
        out[:, cols] = total.astype(out.dtype)
        done.append(pltpu.make_async_copy(out.at[:, cols], out_hbm.at[:, cols], out_sems.at[n]))
        done[-1].start()
    for copy in done:
        copy.wait()


def combine(first, meta, back, sizes, extra):
    rows, width = back.shape
    tokens = meta.shape[1]
    return pl.pallas_call(
        functools.partial(combine_body, sizes, len(extra)),
        out_shape=jax.ShapeDtypeStruct((tokens, width), BF16),
        in_specs=[SMEM, VMEM] + [ANY] * (1 + len(extra)),
        out_specs=ANY,
        scratch_shapes=[pltpu.VMEM(x.shape, x.dtype) for x in extra]
        + [
            pltpu.VMEM((rows, width), BF16),
            pltpu.VMEM((tokens, width), BF16),
            pltpu.SemaphoreType.DMA((1 + len(extra), STEPS)),
            pltpu.SemaphoreType.DMA((STEPS,)),
        ],
        cost_estimate=cost(4 * tokens * rows * width, 2 * rows * width),
        compiler_params=PARAMS,
    )(first, meta, back, *extra)


def per_device(
    conv_value,
    conv_gate,
    taps,
    doc_ids,
    gn_gain,
    gn_shift,
    conv_out,
    residual,
    norm_gain,
    routes,
    route_weight,
    expert_gate,
    expert_up,
    expert_down,
    shared_gate,
    shared_up,
    shared_down,
):
    model_width = residual.shape[1]
    token_count, top_count = routes.shape
    half_devices = lax.axis_size("sp") * lax.axis_size("tp")
    local_experts = expert_gate.shape[0]
    half_experts = local_experts * half_devices
    experts = half_experts * lax.axis_size("half")
    capacity = 2 * token_count * top_count // experts
    half_rows = half_experts * capacity
    first = (lax.axis_index("half").astype(I32) * half_experts).reshape(1)
    core = lax.axis_index("tp").astype(I32).reshape(1)
    sizes = (experts, capacity, top_count)

    ids = doc_ids[None, :]
    gain, shift = gn_gain[None, :], gn_shift[None, :]
    own_edge, own_meta = edge_of(conv_value, conv_gate, ids, routes.T, route_weight.T, ROWS)
    edge = from_behind(own_edge, LINE, 1)
    keep, send = convolve(
        core, conv_value, conv_gate, ids, taps, gain, shift, token_count
    )
    keep, send = convolve_rim(
        core, edge, conv_value, conv_gate, ids, taps, gain, shift, keep, send
    )
    got = lax.ppermute(send, "tp", [(0, 1), (1, 0)])
    mirror_meta = to_mirror(own_meta)
    parcel, stream, normed = project(
        first, core, keep, got, conv_out, residual, norm_gain[None, :], own_meta, sizes, half_rows
    )
    mirror_normed = to_mirror(normed)

    def exchange(rows):
        parcel = rows.reshape(half_devices, local_experts * capacity, model_width)
        arrived = lax.all_to_all(parcel, HALF, split_axis=0, concat_axis=0, tiled=True)
        return arrived.reshape(half_rows, model_width)

    def experts_on(rows):
        split = rows.reshape(half_devices, local_experts, capacity, model_width)
        results = []
        for e in range(local_experts):
            mine = split[:, e].reshape(half_devices * capacity, model_width)
            result = gated_mlp(mine, expert_gate[e], expert_up[e], expert_down[e], (), BF16)
            results.append(result.reshape(half_devices, capacity, model_width))
        return jnp.stack(results, axis=1)

    own_arrived = exchange(parcel)
    mirror_parcel = gather(first, mirror_meta, mirror_normed, sizes, half_rows)
    mirror_arrived = exchange(mirror_parcel)
    base = gated_mlp(normed, shared_gate, shared_up, shared_down, (stream,), F32)
    own_result = experts_on(own_arrived)
    mirror_result = experts_on(mirror_arrived)
    mirror_back = exchange(mirror_result)
    partial = combine(first, mirror_meta, mirror_back, sizes, ())
    other_part = to_mirror(partial)
    own_back = exchange(own_result)
    return combine(first, own_meta, own_back, sizes, (base, other_part))


def solution(mesh):
    sequence_split, core_split = mesh.devices.shape
    folded = Mesh(
        mesh.devices.reshape(2, sequence_split // 2, core_split), ("half", "sp", "tp")
    )
    line, everyone = LINE, LINE + ("tp",)
    return jax.shard_map(
        per_device,
        mesh=folded,
        in_specs=(
            P(line, "tp"),
            P(line, "tp"),
            P(None, "tp"),
            P(line),
            P("tp"),
            P("tp"),
            P(),
            P(everyone, None),
            P(),
            P(everyone, None),
            P(everyone, None),
            P(everyone, None, None),
            P(everyone, None, None),
            P(everyone, None, None),
            P(),
            P(),
            P(),
        ),
        out_specs=P(everyone, None),
        check_vma=False,
    )
```

```python
import functools

import jax
import jax.numpy as jnp
from jax import lax
from jax.experimental import pallas as pl
from jax.experimental.pallas import tpu as pltpu
from jax.sharding import Mesh
from jax.sharding import PartitionSpec as P

LANES = 128


epsilon = 1e-06

HALF = ("sp", "tp")
LINE = ("half", "sp")

F32, BF16, I32 = jnp.float32, jnp.bfloat16, jnp.int32

ROWS = 32
STEPS = 4

VMEM = pl.BlockSpec(memory_space=pltpu.VMEM)
ANY = pl.BlockSpec(memory_space=pl.ANY)
HBM = pl.BlockSpec(memory_space=pltpu.HBM)
PARAMS = pltpu.CompilerParams(vmem_limit_bytes=24 * 2**20)


def from_behind(x, axis, by):
    peers = lax.axis_size(axis)
    pairs = [(i, i + by) for i in range(peers) if 0 <= i + by < peers]
    return lax.ppermute(x, axis, pairs)


def to_mirror(x):
    return lax.ppermute(x, "half", [(0, 1), (1, 0)])


def kept(*arrays):
    return [pltpu.with_memory_space_constraint(x, pltpu.HBM) for x in arrays]


def glu_of(value, gate):
    return (value.astype(F32) * jax.nn.sigmoid(gate.astype(F32))).astype(BF16)


def cost(flops, moved):
    return pl.CostEstimate(
        flops=int(flops), bytes_accessed=int(moved), transcendentals=0
    )


def column_of(row, count, start):
    across = lax.broadcasted_iota(I32, (count, LANES), 1)
    down = lax.broadcasted_iota(I32, (count, LANES), 0)
    picked = jnp.where(across == down + start, row, 0.0)
    return jnp.broadcast_to(jnp.sum(picked, axis=1, keepdims=True), (count, LANES))


def start_copies(pairs, sems, first=0):
    copies = []
    for index, (source, target) in enumerate(pairs):
        copies.append(pltpu.make_async_copy(source, target, sems.at[first + index]))
        copies[-1].start()
    return copies


def edge_body(
    value_hbm,
    gate_hbm,
    ids_hbm,
    routes_hbm,
    weight_hbm,
    edge_ref,
    meta_ref,
    value,
    gate,
    ids,
    routes,
    sems,
):
    rim, channels = value.shape
    positions = value_hbm.shape[0]
    top = routes_hbm.shape[0]
    tail = pl.ds(positions - rim, rim)
    copies = start_copies(
        (
            (value_hbm.at[tail, :], value),
            (gate_hbm.at[tail, :], gate),
            (ids_hbm.at[:, pl.ds(positions - LANES, LANES)], ids),
            (routes_hbm, routes),
            (weight_hbm, meta_ref.at[pl.ds(top, top), :]),
        ),
        sems,
    )
    for copy in copies:
        copy.wait()
    edge_ref[:, pl.ds(0, channels)] = glu_of(value[...], gate[...])
    edge_ref[:, pl.ds(channels, LANES)] = column_of(
        ids[...].astype(F32), rim, LANES - rim
    ).astype(BF16)
    meta_ref[pl.ds(0, top), :] = routes[...].astype(F32)


def edge_of(value, gate, ids, routes, weight, rim):
    channels = value.shape[1]
    top, tokens = routes.shape
    return pl.pallas_call(
        edge_body,
        out_shape=(
            jax.ShapeDtypeStruct((rim, channels + LANES), BF16),
            jax.ShapeDtypeStruct((2 * top, tokens), F32),
        ),
        in_specs=[HBM] * 5,
        out_specs=(VMEM, VMEM),
        scratch_shapes=[
            pltpu.VMEM((rim, channels), BF16),
            pltpu.VMEM((rim, channels), BF16),
            pltpu.VMEM((1, LANES), I32),
            pltpu.VMEM((top, tokens), I32),
            pltpu.SemaphoreType.DMA((5,)),
        ],
        cost_estimate=cost(1e6, 1e5),
        compiler_params=PARAMS,
        name="edge",
    )(*kept(value, gate, ids, routes, weight))


def conv_rows(row, count, rim, width, blocks, glu, ids, weights, gain_ref, shift_ref, store):
    here = ids[pl.ds(row + rim, count), :]
    total = [jnp.zeros((count, LANES), F32) for _ in range(blocks)]
    for tap in range(width):
        past = row + (rim - width + 1 + tap)
        same = ids[pl.ds(past, count), :] == here
        for c in range(blocks):
            weight = weights[pl.ds(tap, 1), pl.ds(c * LANES, LANES)]
            term = weight * glu[c, pl.ds(past, count), :]
            total[c] = total[c] + jnp.where(same, term, 0.0)
    for c in range(blocks):
        lanes = pl.ds(c * LANES, LANES)
        centered = total[c] - jnp.mean(total[c], axis=-1, keepdims=True)
        spread = jnp.mean(centered * centered, axis=-1, keepdims=True)
        scaled = centered * lax.rsqrt(spread + epsilon)
        store(
            lanes,
            jax.nn.silu(scaled * gain_ref[:, lanes] + shift_ref[:, lanes]).astype(BF16),
        )


def conv_body(
    value_hbm,
    gate_hbm,
    ids_hbm,
    taps_hbm,
    gain_hbm,
    shift_hbm,
    keep_ref,
    send_ref,
    head_ref,
    head_ids_ref,
    weights,
    gain_ref,
    shift_ref,
    value,
    gate,
    ids_row,
    taps,
    glu,
    ids,
    sems,
):
    positions, channels = value_hbm.shape
    width = taps_hbm.shape[0]
    blocks = channels // LANES
    rows = ROWS
    tokens = keep_ref.shape[0]
    small = start_copies(
        (
            (ids_hbm, ids_row),
            (taps_hbm, taps),
            (gain_hbm, gain_ref),
            (shift_hbm, shift_ref),
        ),
        sems,
    )
    tiles = []
    for c in range(blocks):
        lanes = pl.ds(c * LANES, LANES)
        tiles.append(
            start_copies(
                (
                    (value_hbm.at[:, lanes], value.at[:, lanes]),
                    (gate_hbm.at[:, lanes], gate.at[:, lanes]),
                ),
                sems,
                4 + 2 * c,
            )
        )
    for copy in small:
        copy.wait()
    weights[pl.ds(0, width), :] = taps[...].astype(F32)
    for start in range(0, positions, LANES):
        row = ids_row[:, pl.ds(start, LANES)].astype(F32)
        ids[pl.ds(start, LANES), :] = column_of(row, LANES, 0)
    for c, pair in enumerate(tiles):
        lanes = pl.ds(c * LANES, LANES)
        for copy in pair:
            copy.wait()
        glu[c] = glu_of(value[:, lanes], gate[:, lanes]).astype(F32)
        head_ref[c] = glu[c, pl.ds(0, rows), :]
    head_ids_ref[...] = ids[pl.ds(0, rows), :]

    core = lax.axis_index("tp")
    parts = positions // tokens
    for out_ref, part in ((send_ref, parts - 1 - core), (keep_ref, core)):

        def step(index, carry, out_ref=out_ref, part=part):
            inside = pl.multiple_of(index * rows, rows)
            row = pl.multiple_of(part * tokens + inside - rows, rows)

            def store(lanes, act):
                out_ref[pl.ds(inside, rows), lanes] = act

            conv_rows(
                row, rows, rows, width, blocks, glu, ids, weights, gain_ref, shift_ref, store
            )
            return carry

        lax.fori_loop((part == 0).astype(I32), tokens // rows, step, 0)


def convolve(value, gate, ids, taps, gain, shift, tokens):
    positions, channels = value.shape
    blocks = channels // LANES
    half = jax.ShapeDtypeStruct((tokens, channels), BF16)
    taps_rows = -(-taps.shape[0] // 8) * 8

    def same(x):
        return jax.ShapeDtypeStruct(x.shape, x.dtype)

    return pl.pallas_call(
        conv_body,
        out_shape=(
            half,
            half,
            jax.ShapeDtypeStruct((blocks, ROWS, LANES), F32),
            jax.ShapeDtypeStruct((ROWS, LANES), F32),
            jax.ShapeDtypeStruct((taps_rows, channels), F32),
            same(gain),
            same(shift),
        ),
        in_specs=[HBM] * 6,
        out_specs=[VMEM] * 7,
        scratch_shapes=[
            pltpu.VMEM((positions, channels), BF16),
            pltpu.VMEM((positions, channels), BF16),
            pltpu.VMEM((1, positions), I32),
            pltpu.VMEM(taps.shape, BF16),
            pltpu.VMEM((blocks, positions, LANES), F32),
            pltpu.VMEM((positions, LANES), F32),
            pltpu.SemaphoreType.DMA((4 + 2 * blocks,)),
        ],
        cost_estimate=cost(6e9, 6 * value.size),
        compiler_params=PARAMS,
        name="conv",
    )(*kept(value, gate, ids, taps, gain, shift))


def rim_body(
    width,
    edge_ref,
    head_ref,
    head_ids_ref,
    weights,
    gain_ref,
    shift_ref,
    keep_in,
    send_in,
    keep_any,
    send_any,
    glu,
    ids,
    act,
    sem,
):
    blocks, rows, _ = head_ref.shape
    channels = blocks * LANES
    ids[pl.ds(0, rows), :] = edge_ref[:, pl.ds(channels, LANES)].astype(F32)
    ids[pl.ds(rows, rows), :] = head_ids_ref[...]
    for c in range(blocks):
        glu[c, pl.ds(0, rows), :] = edge_ref[:, pl.ds(c * LANES, LANES)].astype(F32)
        glu[c, pl.ds(rows, rows), :] = head_ref[c]

    def store(lanes, value):
        act[:, lanes] = value

    conv_rows(0, rows, rows, width, blocks, glu, ids, weights, gain_ref, shift_ref, store)

    core = lax.axis_index("tp")
    for mine, out_any in ((core == 0, keep_any), (core != 0, send_any)):

        @pl.when(mine)
        def _(out_any=out_any):
            copy = pltpu.make_async_copy(act, out_any.at[pl.ds(0, rows), :], sem)
            copy.start()
            copy.wait()


def convolve_rim(edge, head, head_ids, weights, gain, shift, keep, send, width):
    blocks = head.shape[0]
    return pl.pallas_call(
        functools.partial(rim_body, width),
        out_shape=(
            jax.ShapeDtypeStruct(keep.shape, BF16),
            jax.ShapeDtypeStruct(send.shape, BF16),
        ),
        in_specs=[VMEM] * 6 + [ANY] * 2,
        out_specs=(ANY, ANY),
        input_output_aliases={6: 0, 7: 1},
        scratch_shapes=[
            pltpu.VMEM((blocks, 2 * ROWS, LANES), F32),
            pltpu.VMEM((2 * ROWS, LANES), F32),
            pltpu.VMEM((ROWS, blocks * LANES), BF16),
            pltpu.SemaphoreType.DMA,
        ],
        cost_estimate=cost(1e9, 4e5),
        compiler_params=PARAMS,
        name="rim",
    )(edge, head, head_ids, weights, gain, shift, keep, send)


def selection(routes, first, experts, capacity, rows):
    top, tokens = routes.shape
    routes = routes.astype(I32)
    names = lax.broadcasted_iota(I32, (experts, tokens), 0)
    earlier = lax.broadcasted_iota(I32, (tokens, tokens), 0) < lax.broadcasted_iota(
        I32, (tokens, tokens), 1
    )
    earlier = earlier.astype(F32).astype(BF16)
    index = lax.broadcasted_iota(I32, (rows, tokens), 0)
    used = jnp.zeros((experts, 1), F32)
    picks = []
    for k in range(top):
        route = routes[k : k + 1, :]
        chosen = (names == route).astype(F32)
        before = jnp.dot(chosen.astype(BF16), earlier, preferred_element_type=F32) + used
        slot = jnp.sum(chosen * before, axis=0, keepdims=True).astype(I32)
        picks.append(index == (route - first) * capacity + slot)
        used = used + jnp.sum(chosen, axis=1, keepdims=True)
    return picks


def first_expert(experts):
    return lax.axis_index("half") * (experts // lax.axis_size("half"))


def chosen_of(picks):
    return functools.reduce(jnp.logical_or, picks).astype(F32).astype(BF16)


def project_body(
    shape_of,
    meta_ref,
    gain_ref,
    keep_ref,
    got_ref,
    weight_ref,
    residual_ref,
    parcel_hbm,
    stream_ref,
    normed_ref,
    parcel,
    sems,
):
    experts, capacity, top = shape_of
    depth = keep_ref.shape[1]
    width = residual_ref.shape[1]
    core = lax.axis_index("tp")
    mine = pl.multiple_of(core * depth, depth)
    theirs = pl.multiple_of((1 - core) * depth, depth)
    picks = selection(
        meta_ref[pl.ds(0, top), :], first_expert(experts), experts, capacity, parcel.shape[0]
    )
    chosen = chosen_of(picks)
    tile = width // STEPS
    square = 0.0
    for n in range(STEPS):
        cols = pl.ds(n * tile, tile)
        total = jnp.dot(
            keep_ref[...], weight_ref[pl.ds(mine, depth), cols], preferred_element_type=F32
        )
        total = total + jnp.dot(
            got_ref[...], weight_ref[pl.ds(theirs, depth), cols], preferred_element_type=F32
        )
        stream = (residual_ref[:, cols].astype(F32) + total).astype(BF16)
        stream_ref[:, cols] = stream
        wide = stream.astype(F32)
        square = square + jnp.sum(wide * wide, axis=-1, keepdims=True)
    scale = lax.rsqrt(square / width + epsilon)
    back = []
    for n in range(STEPS):
        cols = pl.ds(n * tile, tile)
        normed = (stream_ref[:, cols].astype(F32) * scale * gain_ref[:, cols]).astype(BF16)
        normed_ref[:, cols] = normed
        parcel[:, cols] = jnp.dot(chosen, normed, preferred_element_type=F32).astype(BF16)
        back += start_copies(((parcel.at[:, cols], parcel_hbm.at[:, cols]),), sems, n)
    for copy in back:
        copy.wait()


def project(keep, got, weight, residual, gain, meta, sizes, rows):
    tokens, width = residual.shape
    out = jax.ShapeDtypeStruct((tokens, width), BF16)
    return pl.pallas_call(
        functools.partial(project_body, sizes),
        out_shape=(pltpu.HBM((rows, width), BF16), out, out),
        in_specs=[VMEM] * 6,
        out_specs=[HBM, VMEM, VMEM],
        scratch_shapes=[
            pltpu.VMEM((rows, width), BF16),
            pltpu.SemaphoreType.DMA((STEPS,)),
        ],
        cost_estimate=cost(2 * tokens * weight.size, 2 * weight.size),
        compiler_params=PARAMS,
        name="project",
    )(meta, gain, keep, got, weight, residual)


def gather_body(shape_of, meta_ref, rows_ref, parcel_ref):
    experts, capacity, top = shape_of
    picks = selection(
        meta_ref[pl.ds(0, top), :], first_expert(experts), experts, capacity, parcel_ref.shape[0]
    )
    chosen = chosen_of(picks)
    tile = rows_ref.shape[1] // STEPS
    for n in range(STEPS):
        cols = pl.ds(n * tile, tile)
        parcel_ref[:, cols] = jnp.dot(
            chosen, rows_ref[:, cols], preferred_element_type=F32
        ).astype(BF16)


def gather(meta, rows, sizes, count):
    tokens, width = rows.shape
    return pl.pallas_call(
        functools.partial(gather_body, sizes),
        out_shape=jax.ShapeDtypeStruct((count, width), BF16),
        in_specs=[VMEM, VMEM],
        out_specs=VMEM,
        cost_estimate=cost(2 * count * tokens * width, 2 * (count + tokens) * width),
        compiler_params=PARAMS,
        name="gather",
    )(meta, rows)


def expert_body(
    rows_ref, gate_ref, up_hbm, down_hbm, out_hbm, up, down, hidden, out, up_sems, sems, out_sems
):
    inner = gate_ref.shape[1]
    width = out.shape[1]
    half = inner // 2
    halves = [pl.ds(n * half, half) for n in range(2)]
    first = start_copies([(up_hbm.at[:, cols], up.at[:, cols]) for cols in halves], up_sems)
    second = stream_in(down_hbm, down, sems)
    rows = rows_ref[...]
    for cols, copy in zip(halves, first):
        gate = jnp.dot(rows, gate_ref[:, cols], preferred_element_type=F32)
        copy.wait()
        raised = jnp.dot(rows, up[:, cols], preferred_element_type=F32)
        hidden[:, cols] = (jax.nn.silu(gate) * raised).astype(BF16)
    tile = width // STEPS
    back = []
    for n, copy in enumerate(second):
        cols = pl.ds(n * tile, tile)
        copy.wait()
        out[:, cols] = jnp.dot(hidden[...], down[:, cols], preferred_element_type=F32).astype(BF16)
        back += start_copies(((out.at[:, cols], out_hbm.at[:, cols]),), out_sems, n)
    for copy in back:
        copy.wait()


def expert(rows, gate, up, down):
    count, width = rows.shape
    inner = gate.shape[1]
    return pl.pallas_call(
        expert_body,
        out_shape=pltpu.HBM((count, width), BF16),
        in_specs=[VMEM] * 2 + [HBM] * 2,
        out_specs=HBM,
        scratch_shapes=[
            pltpu.VMEM(up.shape, BF16),
            pltpu.VMEM(down.shape, BF16),
            pltpu.VMEM((count, inner), BF16),
            pltpu.VMEM((count, width), BF16),
            pltpu.SemaphoreType.DMA((2,)),
            pltpu.SemaphoreType.DMA((STEPS,)),
            pltpu.SemaphoreType.DMA((STEPS,)),
        ],
        cost_estimate=cost(6 * count * width * inner, 6 * width * inner),
        compiler_params=PARAMS,
        name="expert",
    )(rows, gate, *kept(up, down))


def mlp_body(
    steps,
    rows_hbm,
    gate_hbm,
    up_hbm,
    down_hbm,
    *rest,
):
    extra = rest[:-11]
    (out_hbm, rows, gate, up, down, total_gate, total_up, hidden, out, in_sems, out_sems) = rest[
        -11:
    ]
    depth = gate.shape[0] // steps
    tile = down.shape[1] // steps
    rows_copy = pltpu.make_async_copy(rows_hbm, rows, in_sems.at[0])
    rows_copy.start()
    wide, narrow = [], []
    for n in range(steps):
        part = pl.ds(n * depth, depth)
        pair = (
            pltpu.make_async_copy(gate_hbm.at[part, :], gate.at[part, :], in_sems.at[1 + 3 * n]),
            pltpu.make_async_copy(up_hbm.at[part, :], up.at[part, :], in_sems.at[2 + 3 * n]),
        )
        for copy in pair:
            copy.start()
        wide.append(pair)
    for n in range(steps):
        cols = pl.ds(n * tile, tile)
        copy = pltpu.make_async_copy(down_hbm.at[:, cols], down.at[:, cols], in_sems.at[3 + 3 * n])
        copy.start()
        narrow.append(copy)
    rows_copy.wait()
    for n, pair in enumerate(wide):
        part = pl.ds(n * depth, depth)
        for copy, weight, total in zip(pair, (gate, up), (total_gate, total_up)):
            copy.wait()
            product = jnp.dot(rows[:, part], weight[part, :], preferred_element_type=F32)
            total[...] = product if n == 0 else total[...] + product
    hidden[...] = (jax.nn.silu(total_gate[...]) * total_up[...]).astype(BF16)
    back = []
    for n, copy in enumerate(narrow):
        cols = pl.ds(n * tile, tile)
        copy.wait()
        result = jnp.dot(hidden[...], down[:, cols], preferred_element_type=F32)
        for ref in extra:
            result = result + ref[:, cols].astype(F32)
        out[:, cols] = result.astype(out.dtype)
        copy = pltpu.make_async_copy(out.at[:, cols], out_hbm.at[:, cols], out_sems.at[n])
        copy.start()
        back.append(copy)
    for copy in back:
        copy.wait()


def gated_mlp(rows, gate, up, down, extra, dtype):
    count, width = rows.shape
    inner = gate.shape[-1]
    steps = STEPS
    return pl.pallas_call(
        functools.partial(mlp_body, steps),
        out_shape=pltpu.HBM((count, width), dtype),
        in_specs=[ANY] + [HBM] * 3 + [VMEM] * len(extra),
        out_specs=ANY,
        scratch_shapes=[
            pltpu.VMEM((count, width), rows.dtype),
            pltpu.VMEM((width, inner), gate.dtype),
            pltpu.VMEM((width, inner), up.dtype),
            pltpu.VMEM((inner, width), down.dtype),
            pltpu.VMEM((count, inner), F32),
            pltpu.VMEM((count, inner), F32),
            pltpu.VMEM((count, inner), BF16),
            pltpu.VMEM((count, width), dtype),
            pltpu.SemaphoreType.DMA((1 + 3 * steps,)),
            pltpu.SemaphoreType.DMA((steps,)),
        ],
        cost_estimate=cost(6 * count * width * inner, 6 * width * inner),
        compiler_params=PARAMS,
    )(rows, *kept(gate, up, down), *extra)


def stream_in(source, target, sems):
    tile = target.shape[1] // STEPS
    tiles = [pl.ds(n * tile, tile) for n in range(STEPS)]
    return start_copies([(source.at[:, cols], target.at[:, cols]) for cols in tiles], sems)


def weigh(shape_of, meta_ref, rows):
    experts, capacity, top = shape_of
    picks = selection(meta_ref[pl.ds(0, top), :], first_expert(experts), experts, capacity, rows)
    table = jnp.zeros((rows, meta_ref.shape[1]), F32)
    for k, pick in enumerate(picks):
        table = table + jnp.where(pick, meta_ref[pl.ds(top + k, 1), :], 0.0)
    table = table.T
    high = table.astype(BF16)
    return high, (table - high.astype(F32)).astype(BF16)


def partial_body(shape_of, meta_ref, back_ref, out_ref):
    high, low = weigh(shape_of, meta_ref, back_ref.shape[0])
    tile = back_ref.shape[1] // STEPS
    for n in range(STEPS):
        cols = pl.ds(n * tile, tile)
        total = jnp.dot(high, back_ref[:, cols], preferred_element_type=F32)
        total = total + jnp.dot(low, back_ref[:, cols], preferred_element_type=F32)
        out_ref[:, cols] = total.astype(BF16)


def partial_sum(meta, back, sizes):
    rows, width = back.shape
    tokens = meta.shape[1]
    return pl.pallas_call(
        functools.partial(partial_body, sizes),
        out_shape=jax.ShapeDtypeStruct((tokens, width), BF16),
        in_specs=[VMEM, VMEM],
        out_specs=VMEM,
        cost_estimate=cost(4 * tokens * rows * width, 2 * rows * width),
        compiler_params=PARAMS,
        name="partial",
    )(meta, back)


def final_body(
    shape_of, meta_ref, back_ref, other_ref, base_any, out_hbm, base, out, in_sems, sems
):
    arrivals = stream_in(base_any, base, in_sems)
    high, low = weigh(shape_of, meta_ref, back_ref.shape[0])
    tile = back_ref.shape[1] // STEPS
    done = []
    for n in range(STEPS):
        cols = pl.ds(n * tile, tile)
        total = jnp.dot(high, back_ref[:, cols], preferred_element_type=F32)
        total = total + jnp.dot(low, back_ref[:, cols], preferred_element_type=F32)
        arrivals[n].wait()
        total = total + other_ref[:, cols].astype(F32) + base[:, cols]
        out[:, cols] = total.astype(BF16)
        done += start_copies(((out.at[:, cols], out_hbm.at[:, cols]),), sems, n)
    for copy in done:
        copy.wait()


def final_sum(meta, back, other, base, sizes):
    rows, width = back.shape
    tokens = meta.shape[1]
    return pl.pallas_call(
        functools.partial(final_body, sizes),
        out_shape=jax.ShapeDtypeStruct((tokens, width), BF16),
        in_specs=[VMEM] * 3 + [HBM],
        out_specs=HBM,
        scratch_shapes=[
            pltpu.VMEM((tokens, width), F32),
            pltpu.VMEM((tokens, width), BF16),
            pltpu.SemaphoreType.DMA((STEPS,)),
            pltpu.SemaphoreType.DMA((STEPS,)),
        ],
        cost_estimate=cost(4 * tokens * rows * width, 2 * rows * width),
        compiler_params=PARAMS,
        name="final",
    )(meta, back, other, *kept(base))


def per_device(
    conv_value,
    conv_gate,
    taps,
    doc_ids,
    gn_gain,
    gn_shift,
    conv_out,
    residual,
    norm_gain,
    routes,
    route_weight,
    expert_gate,
    expert_up,
    expert_down,
    shared_gate,
    shared_up,
    shared_down,
):
    model_width = residual.shape[1]
    token_count, top_count = routes.shape
    half_devices = lax.axis_size("sp") * lax.axis_size("tp")
    local_experts = expert_gate.shape[0]
    half_experts = local_experts * half_devices
    experts = half_experts * lax.axis_size("half")
    capacity = 2 * token_count * top_count // experts
    half_rows = half_experts * capacity
    sizes = (experts, capacity, top_count)

    ids = doc_ids[None, :]
    gain, shift = gn_gain[None, :], gn_shift[None, :]
    own_edge, own_meta = edge_of(conv_value, conv_gate, ids, routes.T, route_weight.T, ROWS)
    edge = from_behind(own_edge, LINE, 1)
    keep, send, head, head_ids, weights, gain, shift = convolve(
        conv_value, conv_gate, ids, taps, gain, shift, token_count
    )
    keep, send = convolve_rim(
        edge, head, head_ids, weights, gain, shift, keep, send, taps.shape[0]
    )
    got = lax.ppermute(send, "tp", [(0, 1), (1, 0)])
    mirror_meta = to_mirror(own_meta)
    parcel, stream, normed = project(
        keep, got, conv_out, residual, norm_gain[None, :], own_meta, sizes, half_rows
    )
    mirror_normed = to_mirror(normed)

    def exchange(rows):
        parcel = rows.reshape(half_devices, local_experts * capacity, model_width)
        arrived = lax.all_to_all(parcel, HALF, split_axis=0, concat_axis=0, tiled=True)
        return arrived.reshape(half_rows, model_width)

    def experts_on(rows):
        split = rows.reshape(half_devices, local_experts, capacity, model_width)
        results = []
        for e in range(local_experts):
            mine = split[:, e].reshape(half_devices * capacity, model_width)
            results.append(
                expert(mine, expert_gate[e], expert_up[e], expert_down[e]).reshape(half_devices, capacity, model_width)
            )
        return jnp.stack(results, axis=1)

    own_arrived = exchange(parcel)
    base = gated_mlp(normed, shared_gate, shared_up, shared_down, (stream,), F32)
    mirror_parcel = gather(mirror_meta, mirror_normed, sizes, half_rows)
    mirror_arrived = exchange(mirror_parcel)
    mirror_result = experts_on(mirror_arrived)
    mirror_back = exchange(mirror_result)
    own_result = experts_on(own_arrived)
    partial = partial_sum(mirror_meta, mirror_back, sizes)
    other_part = to_mirror(partial)
    own_back = exchange(own_result)
    return final_sum(own_meta, own_back, other_part, base, sizes)


def solution(mesh):
    sequence_split, core_split = mesh.devices.shape
    folded = Mesh(
        mesh.devices.reshape(2, sequence_split // 2, core_split), ("half", "sp", "tp")
    )
    line, everyone = LINE, LINE + ("tp",)
    return jax.shard_map(
        per_device,
        mesh=folded,
        in_specs=(
            P(line, "tp"),
            P(line, "tp"),
            P(None, "tp"),
            P(line),
            P("tp"),
            P("tp"),
            P(),
            P(everyone, None),
            P(),
            P(everyone, None),
            P(everyone, None),
            P(everyone, None, None),
            P(everyone, None, None),
            P(everyone, None, None),
            P(),
            P(),
            P(),
        ),
        out_specs=P(everyone, None),
        check_vma=False,
    )
```
